32 devices in a mesh: kv: 8 (over z, y), tp: 4 (over x, core).
Axes of the slice: x: 2, y: 2, z: 4, core: 2. Of those that a mesh axis runs over, the one named last changes fastest.
Arguments:
- residual_in: bfloat16 [64, 2048], P(None, ('kv', 'tp')), may hold values from -14 to 14
- delta_state: float32 [64, 32, 128, 128], P('kv', 'tp'), may hold values from -1 to 1
- norm_gain_first: float32 [2048], P('kv'), may hold values from 0.1 to 1.9
- gate_first: bfloat16 [2048, 5632], P('kv', 'tp'), may hold values from -0.125 to 0.125
- up_first: bfloat16 [2048, 5632], P('kv', 'tp'), may hold values from -0.125 to 0.125
- down_first: bfloat16 [5632, 2048], P('tp', 'kv'), may hold values from -0.15625 to 0.15625
- norm_gain_mixer: float32 [2048], P('kv'), may hold values from 0.1 to 1.9
- query_weight: bfloat16 [2048, 2048], P('kv', 'tp'), may hold values from -0.125 to 0.125
- key_weight: bfloat16 [2048, 2048], P('kv', 'tp'), may hold values from -0.125 to 0.125
- value_weight: bfloat16 [2048, 4096], P('kv', 'tp'), may hold values from -0.125 to 0.125
- output_gate_weight: bfloat16 [2048, 4096], P('kv', 'tp'), may hold values from -0.125 to 0.125
- beta_weight: bfloat16 [2048, 32], P('kv'), may hold values from -0.125 to 0.125
- decay_weight: bfloat16 [2048, 32], P('kv'), may hold values from -0.125 to 0.125
- decay_rate: float32 [32], P('tp'), may hold values from -2.3 to 1.1
- decay_bias: float32 [32], P('tp'), may hold values from -1 to 1
- head_gain: float32 [128], replicated, may hold values from 0.1 to 1.9
- out_weight: bfloat16 [4096, 2048], P('tp', 'kv'), may hold values from -0.125 to 0.125
- norm_gain_second: float32 [2048], P('kv'), may hold values from 0.1 to 1.9
- gate_second: bfloat16 [2048, 5632], P('kv', 'tp'), may hold values from -0.125 to 0.125
- up_second: bfloat16 [2048, 5632], P('kv', 'tp'), may hold values from -0.125 to 0.125
- down_second: bfloat16 [5632, 2048], P('tp', 'kv'), may hold values from -0.15625 to 0.15625
Outputs:
- residual_out: bfloat16 [64, 2048], P(None, ('kv', 'tp'))
- delta_state_out: float32 [64, 32, 128, 128], P('kv', 'tp')
The draws below stay inside these ranges and needn't reach their ends.
All inputs are finite; a program needn't handle non-finite values.
Results may differ from the reference program's by a relative error of at most 0.03.
Values may be sent and summed in bfloat16 or wider, within the bound.
A program may use at most 64 MiB of HBM per device.

```python
import jax
import jax.numpy as jnp
from jax import lax

D = 2048
FF = 5632
K_HEADS = 16
HEAD = 128
V_HEADS = 32
KW = 2048
VW = 4096
BATCH = 64
N_TP = 4


def draw_residual_in(key, part):
    keys = jax.random.split(key, 4)
    region = jnp.arange(D, dtype=jnp.int32) // (D // 8)
    region_scale = jnp.exp(jax.random.uniform(keys[0], (8,), jnp.float32, -0.6, 0.6))
    column_scale = region_scale[region] * jnp.exp(jax.random.uniform(keys[1], (D,), jnp.float32, -0.2, 0.2))
    base = jnp.clip(jax.random.normal(keys[2], (BATCH, D), jnp.float32), -4.0, 4.0)
    row_scale = jnp.exp(jax.random.uniform(keys[3], (BATCH, 1), jnp.float32, -0.4, 0.4))
    return (base * row_scale * column_scale[None, :]).astype(jnp.bfloat16)


def shard_levels(own_key, dims, cuts, smallest, largest):
    loudness, own = 1.0, jax.random.fold_in(own_key, 6)
    for dim, shards_of in cuts:
        draws = jnp.exp(jax.random.uniform(jax.random.fold_in(own, dim), (shards_of,), jnp.float32, smallest / len(cuts), largest / len(cuts)))
        loudness = loudness * jnp.repeat(draws, dims[dim] // shards_of).reshape([-1 if axis == dim else 1 for axis in range(len(dims))])
    return loudness


def bell_draw(rng, dims, spread, reach, cuts=(), kind=jnp.bfloat16):
    factor_of = shard_levels(rng, dims, cuts, -0.22, 0.18) if cuts else 1.0
    result = jax.random.normal(rng, dims, jnp.float32) * spread * factor_of
    return jnp.minimum(jnp.maximum(result, -reach), reach).astype(kind)


def setup_inputs(seed: int = 0) -> dict:
    key_list = jax.random.split(jax.random.key(seed), 22)
    return {
        "residual_in": draw_residual_in(jax.random.fold_in(key_list[21], 71), 0),
        "delta_state": bell_draw(key_list[1], (BATCH, V_HEADS, HEAD, HEAD), 0.2, 1.0, ((0, 8), (1, 4)), jnp.float32),
        "norm_gain_first": jnp.clip(1.0 + 0.18 * jax.random.normal(key_list[2], (D,), jnp.float32), 0.1, 1.9),
        "gate_first": bell_draw(key_list[3], (D, FF), D ** -0.5, 0.125, ((0, 8), (1, 4))),
        "up_first": bell_draw(key_list[4], (D, FF), D ** -0.5, 0.125, ((0, 8), (1, 4))),
        "down_first": bell_draw(key_list[5], (FF, D), (FF // 4) ** -0.5, 0.15625, ((0, 4), (1, 8))),
        "norm_gain_mixer": jnp.clip(1.0 + 0.18 * jax.random.normal(key_list[6], (D,), jnp.float32), 0.1, 1.9),
        "query_weight": bell_draw(key_list[7], (D, KW), D ** -0.5, 0.125, ((0, 8), (1, 4))),
        "key_weight": bell_draw(key_list[8], (D, KW), D ** -0.5, 0.125, ((0, 8), (1, 4))),
        "value_weight": bell_draw(key_list[9], (D, VW), D ** -0.5, 0.125, ((0, 8), (1, 4))),
        "output_gate_weight": bell_draw(key_list[10], (D, VW), D ** -0.5, 0.125, ((0, 8), (1, 4))),
        "beta_weight": bell_draw(key_list[11], (D, V_HEADS), D ** -0.5, 0.125, ((0, 8),)),
        "decay_weight": bell_draw(key_list[12], (D, V_HEADS), D ** -0.5, 0.125, ((0, 8),)),
        "decay_rate": jnp.clip(-2.3 + 3.4 * jax.random.uniform(key_list[13], (V_HEADS,), jnp.float32) ** shard_levels(key_list[13], (V_HEADS,), ((0, 4),), -0.2, 0.2), -2.3, 1.1),
        "decay_bias": jnp.clip(jax.random.uniform(key_list[14], (V_HEADS,), jnp.float32, -1.0, 1.0) * shard_levels(key_list[14], (V_HEADS,), ((0, 4),), -0.4, 0.0), -1.0, 1.0),
        "head_gain": jnp.clip(1.0 + 0.18 * jax.random.normal(key_list[15], (HEAD,), jnp.float32), 0.1, 1.9),
        "out_weight": bell_draw(key_list[16], (VW, D), (VW // 2) ** -0.5, 0.125, ((0, 4), (1, 8))),
        "norm_gain_second": jnp.clip(1.0 + 0.18 * jax.random.normal(key_list[17], (D,), jnp.float32), 0.1, 1.9),
        "gate_second": bell_draw(key_list[18], (D, FF), D ** -0.5, 0.125, ((0, 8), (1, 4))),
        "up_second": bell_draw(key_list[19], (D, FF), D ** -0.5, 0.125, ((0, 8), (1, 4))),
        "down_second": bell_draw(key_list[20], (FF, D), (FF // 4) ** -0.5, 0.15625, ((0, 4), (1, 8))),
    }


epsilon = 1e-06

def head_sums(left_side, right_side):
    left_parts = left_side.reshape(left_side.shape[0], N_TP, -1).astype(jnp.float32)
    weights = right_side.reshape(N_TP, -1, right_side.shape[1]).astype(jnp.float32)
    pieces = jnp.einsum('btf,tfd->tbd', left_parts, weights)
    rounded = lax.optimization_barrier(pieces.astype(jnp.bfloat16))
    return lax.optimization_barrier(jnp.sum(rounded.astype(jnp.float32), axis=0))

def norm_parts(residual, norm_gain):
    as_float = residual.astype(jnp.float32)
    rowscale = lax.rsqrt(lax.optimization_barrier(jnp.sum(as_float * as_float, axis=1, keepdims=True)) / D + epsilon)
    scaled = (as_float * norm_gain).astype(jnp.bfloat16)
    return (as_float, rowscale, scaled)

def half_ffn(residual, norm_gain, gate_weight, up_weight, down_weight):
    as_float, rowscale, scaled = norm_parts(residual, norm_gain)
    gate_act = jnp.dot(scaled, gate_weight, preferred_element_type=jnp.float32) * rowscale
    up_act = jnp.dot(scaled, up_weight, preferred_element_type=jnp.float32) * rowscale
    hidden = (jax.nn.silu(gate_act) * up_act).astype(jnp.bfloat16)
    branch = head_sums(hidden, down_weight)
    return (as_float + 0.5 * branch).astype(jnp.bfloat16)

def unit_heads(projected, head_size):
    activated = jax.nn.silu(projected).reshape(projected.shape[0], -1, head_size)
    return activated * lax.rsqrt(lax.optimization_barrier(jnp.sum(activated * activated, axis=-1, keepdims=True)) + epsilon)

def delta_step(old_state, key_rows, queries, values, beta_gate, decay_gate):
    faded_state = old_state * decay_gate[:, :, None, None]
    predicted = jnp.einsum('rhab,rha->rhb', faded_state, key_rows, precision=lax.Precision.HIGHEST)
    correction = beta_gate[:, :, None] * (values - predicted)
    updated = faded_state + key_rows[:, :, :, None] * correction[:, :, None, :]
    reading = jnp.einsum('rhab,rha->rhb', updated, queries, precision=lax.Precision.HIGHEST)
    return (updated, reading)

def advance(inputs):
    return delta_step(*inputs)

def reference(residual_in, delta_state, norm_gain_first, gate_first, up_first, down_first, norm_gain_mixer, query_weight, key_weight, value_weight, output_gate_weight, beta_weight, decay_weight, decay_rate, decay_bias, head_gain, out_weight, norm_gain_second, gate_second, up_second, down_second):
    after_first = half_ffn(residual_in, norm_gain_first, gate_first, up_first, down_first)
    as_float, rowscale, scaled = norm_parts(after_first, norm_gain_mixer)

    def project(weight):
        return jnp.dot(scaled, weight, preferred_element_type=jnp.float32) * rowscale
    repeat_count = V_HEADS // K_HEADS
    queries = jnp.repeat(unit_heads(project(query_weight), HEAD) * HEAD ** (-0.5), repeat_count, axis=1)
    key_rows = jnp.repeat(unit_heads(project(key_weight), HEAD), repeat_count, axis=1)
    values = jax.nn.silu(project(value_weight)).reshape(BATCH, V_HEADS, HEAD)
    out_gate = jax.nn.silu(project(output_gate_weight)).reshape(BATCH, V_HEADS, HEAD)
    beta_gate = jax.nn.sigmoid(project(beta_weight))
    decay_gate = jnp.exp(-jnp.exp(decay_rate)[None, :] * jax.nn.softplus(project(decay_weight) + decay_bias[None, :]))
    groups = BATCH // 8
    stacked = tuple((item.reshape((groups, BATCH // groups) + item.shape[1:]) for item in (delta_state, key_rows, queries, values, beta_gate, decay_gate)))
    new_state, reading = lax.map(advance, stacked)
    new_state = new_state.reshape(BATCH, V_HEADS, HEAD, HEAD)
    reading = reading.reshape(BATCH, V_HEADS, HEAD)
    normed = reading * lax.rsqrt(lax.optimization_barrier(jnp.mean(reading * reading, axis=-1, keepdims=True)) + epsilon)
    normed = (normed * head_gain * out_gate).reshape(BATCH, VW).astype(jnp.bfloat16)
    after_mixer = (as_float + head_sums(normed, out_weight)).astype(jnp.bfloat16)
    residual_out = half_ffn(after_mixer, norm_gain_second, gate_second, up_second, down_second)
    return (residual_out, new_state)
```

```python
import functools

import jax
import jax.numpy as jnp
from jax import lax
from jax.experimental import pallas as pl
from jax.experimental.pallas import tpu as pltpu
from jax.sharding import PartitionSpec as P

EPS = 1e-06
GROUP = 8
LANES = 128
BF16 = jnp.bfloat16
F32 = jnp.float32
ns = jax.named_scope


def pad_lanes(size):
    return -(-size // LANES) * LANES


def silu(v):
    return v / (1.0 + jnp.exp(-v))


def dot(a, b):
    return jnp.dot(a, b, preferred_element_type=F32)


def dot_first(a, b):
    return lax.dot_general(a, b, (((0,), (0,)), ((), ())), preferred_element_type=F32)


def place(rows, cols, shift):
    row = lax.broadcasted_iota(jnp.int32, (rows, cols), 0)
    col = lax.broadcasted_iota(jnp.int32, (rows, cols), 1)
    return jnp.where(col == row + shift, 1.0, 0.0).astype(F32).astype(BF16)


def kernel(
    n_kv,
    n_tp,
    res_ref,
    gain_first_ref,
    gain_mixer_ref,
    gain_second_ref,
    beta_ref,
    decay_ref,
    rate_ref,
    bias_ref,
    head_gain_ref,
    state_hbm,
    gate1_hbm,
    up1_hbm,
    down1_hbm,
    wq_hbm,
    wk_hbm,
    wv_hbm,
    wo_hbm,
    out_hbm,
    gate2_hbm,
    up2_hbm,
    down2_hbm,
    res_out_ref,
    state,
    gate1,
    up1,
    down1,
    wq,
    wk,
    wv,
    wo,
    wout,
    gate2,
    up2,
    down2,
    res_all,
    s1a,
    r1a,
    s1b,
    r1b,
    hid1,
    par1,
    sma,
    rma,
    smb,
    rmb,
    smc,
    rmc,
    nrm,
    parm,
    s2a,
    r2a,
    s2b,
    r2b,
    hid2,
    fin_send,
    fin_recv,
    qk_rows,
    val_rows,
    dec_rows,
    pred_rows,
    read_rows,
    w_sem,
    in_sem,
    send_sem,
    recv_sem,
):
    kv = lax.axis_index("kv")
    tp = lax.axis_index("tp")
    batch, piece = res_ref.shape
    depth = gate1.shape[0]
    width = depth * n_kv
    own_rows = batch // n_kv
    heads = state.shape[1]
    size = state.shape[2]
    key_cols = wq.shape[1]
    key_heads = key_cols // size
    repeat = heads // key_heads
    half = n_kv // 2
    groups = n_kv // GROUP

    turned = lax.rem(kv + GROUP - 2, GROUP)
    my_c = kv // GROUP
    my_s = turned // 4
    my_e = lax.rem(turned, 4) // 2
    my_b = lax.rem(turned, 2)
    my_j = my_c * 4 + my_e * 2 + my_b

    def device_at(c, stream, e, b):
        return c * GROUP + lax.rem(stream * 4 + e * 2 + b + 2, GROUP)

    def start_of(stream, j):
        return ((j // 4) * GROUP + (stream * 4 + j % 4 + 2) % GROUP) * own_rows

    def rows_of(value, stream):
        parts = [value[start_of(stream, j) : start_of(stream, j) + own_rows] for j in range(half)]
        return jnp.concatenate(parts, axis=0)

    weight_pairs = (
        (gate1_hbm, gate1),
        (up1_hbm, up1),
        (down1_hbm, down1),
        (wq_hbm, wq),
        (wk_hbm, wk),
        (wv_hbm, wv),
        (wo_hbm, wo),
        (out_hbm, wout),
        (gate2_hbm, gate2),
        (up2_hbm, up2),
        (down2_hbm, down2),
    )
    loads = [
        pltpu.make_async_copy(src, dst, w_sem.at[i]) for i, (src, dst) in enumerate(weight_pairs)
    ]
    for load in loads[:7]:
        load.start()

    barrier = pltpu.get_barrier_semaphore()
    for off in range(1, n_tp):
        pl.semaphore_signal(
            barrier,
            inc=1,
            device_id={"tp": lax.rem(tp + off, n_tp)},
            device_id_type=pl.DeviceIdType.MESH,
        )
    for off in range(1, n_kv):
        pl.semaphore_signal(
            barrier,
            inc=1,
            device_id={"kv": lax.rem(kv + off, n_kv)},
            device_id_type=pl.DeviceIdType.MESH,
        )
    with ns("barrier"):
        pl.semaphore_wait(barrier, n_tp - 1 + n_kv - 1)

    pending = []

    def remote(event, index, src, dst, axis, peer):
        return pltpu.make_async_remote_copy(
            src_ref=src,
            dst_ref=dst,
            send_sem=send_sem.at[event, index],
            recv_sem=recv_sem.at[event, index],
            device_id={axis: peer},
            device_id_type=pl.DeviceIdType.MESH,
        )

    def send_tp(event, src_of, dst_of):
        copies = []
        for off in range(1, n_tp):
            peer = lax.rem(tp + off, n_tp)
            copy = remote(event, off, src_of(off), dst_of(off), "tp", peer)
            copy.start()
            pending.append((copy, None))
            copies.append(copy)
        return copies

    steps = [(dc, de, db) for dc in range(groups) for de in (1, 0) for db in (1, 0)]

    def each_kv(stream, make):
        turn = lax.rem(stream + 2 - my_s, 2)
        for dc, de, db in steps:
            c, e, b = lax.rem(my_c + dc, groups), lax.rem(my_e + de, 2), lax.rem(my_b + db, 2)
            index = dc * GROUP + turn * 4 + de * 2 + db
            copy = make(index, device_at(c, stream, e, b), c * 4 + e * 2 + b)
            if (dc, de, db) == (0, 0, 0):
                pl.when(my_s != stream)(copy.start)
                pending.append((copy, stream))
            else:
                copy.start()
                pending.append((copy, None))

    def scatter(event, stream, sends, receives):
        each_kv(
            stream,
            lambda index, peer, j: remote(
                event, index, sends.at[stream, j], receives.at[index], "kv", peer
            ),
        )

    def collect(event, sends, receives):
        total = sends[my_s, my_j].astype(F32)
        for index in range(1, n_kv):
            remote(event, index, receives.at[index], receives.at[index], "kv", kv).wait_recv()
            total = total + receives[index].astype(F32)
        return total

    def spread(event, slots):
        own = slots.at[my_s, my_j]
        for stream in range(2):
            each_kv(stream, lambda index, peer, j: remote(event, index, own, own, "kv", peer))

    def arrive(event, stream, slots):
        turn = lax.rem(my_s + 2 - stream, 2)
        for dc, de, db in reversed(steps):
            index = dc * GROUP + turn * 4 + de * 2 + db
            copy = remote(event, index, slots.at[stream, 0], slots.at[stream, 0], "kv", kv)
            if (dc, de, db) == (0, 0, 0):
                pl.when(my_s != stream)(copy.wait_recv)
            else:
                copy.wait_recv()

    def put(ref, stream, offset, value):
        cols = value.shape[1]
        ref[stream, :, :, offset : offset + cols] = value.reshape(half, own_rows, cols).astype(BF16)

    def square_lanes(residual):
        squares = jnp.sum(residual * residual, axis=1, keepdims=True)
        high = squares.astype(BF16).astype(F32)
        lane = lax.broadcasted_iota(jnp.int32, (residual.shape[0], LANES), 1)
        return jnp.where(lane == 64, high, jnp.where(lane == 65, squares - high, 0.0))

    def row_scale(extra):
        squares = extra[:, 64:65] + extra[:, 65:66]
        return lax.rsqrt(squares / width + EPS)

    def flat(slots, stream):
        both = slots[stream].astype(F32)
        return both.reshape(half * own_rows, both.shape[2]).astype(BF16)

    def share(event, stream, value, slots):
        slots[stream, tp] = value.astype(BF16)
        own = slots.at[stream, tp]
        return send_tp(event, lambda off: own, lambda off: own)

    def join(copies, stream, slots):
        for copy in copies:
            copy.wait_recv()
        total = slots[stream, 0].astype(F32)
        for other in range(1, n_tp):
            total = total + slots[stream, other].astype(F32)
        return total

    def ffn_in(event, stream, residual, gain_ref, w_gate, w_up, bufs):
        send_a, recv_a, send_b, recv_b = bufs
        up_end = pad_lanes(w_gate.shape[1])
        scaled = (residual * gain_ref[...]).astype(BF16)
        put(send_a, stream, 0, dot(scaled, w_gate[...]))
        scatter(event, stream, send_a, recv_a)
        put(send_b, stream, 0, dot(scaled, w_up[...]))
        put(send_b, stream, up_end, square_lanes(residual))
        scatter(event + 1, stream, send_b, recv_b)

    def ffn_mid(event, bufs, hid):
        send_a, recv_a, send_b, recv_b = bufs
        hidden_cols = hid.shape[-1]
        up_end = pad_lanes(hidden_cols)
        with ns("f_rs_a"):
            gate_sum = collect(event, send_a, recv_a)[:, :hidden_cols]
        with ns("f_rs_b"):
            rest = collect(event + 1, send_b, recv_b)
        scale = row_scale(rest[:, up_end:])
        hidden = (silu(gate_sum * scale) * (rest[:, :hidden_cols] * scale)).astype(BF16)
        hid[my_s, my_j] = hidden
        spread(event + 2, hid)

    copies = send_tp(0, lambda off: res_ref, lambda off: res_all.at[tp])
    for load in loads[7:]:
        load.start()
    for row in range(own_rows):
        pltpu.make_async_copy(state_hbm.at[row], state.at[row], in_sem.at[row]).start()
    decay_exp = jnp.exp(rate_ref[...])
    extra_weight = (
        dot_first(beta_ref[...], place_heads(beta_ref.shape[0], tp * heads, 0, heads))
        + dot_first(decay_ref[...], place_heads(beta_ref.shape[0], tp * heads, heads, heads))
    ).astype(BF16)
    whole = dot(res_ref[...], place(piece, depth, tp * piece))
    with ns("tp_gather"):
        for off in range(1, n_tp):
            copies[off - 1].wait_recv()
            source = lax.rem(tp + n_tp - off, n_tp)
            whole = whole + dot(res_all[source], place(piece, depth, source * piece))

    first_bufs = (s1a, r1a, s1b, r1b)
    residual = [rows_of(whole, stream) for stream in range(2)]
    loads[0].wait()
    loads[1].wait()
    with ns("f1_in"):
        for stream in range(2):
            ffn_in(1, stream, residual[stream], gain_first_ref, gate1, up1, first_bufs)
    ffn_mid(1, first_bufs, hid1)
    loads[2].wait()
    shared = []
    for stream in range(2):
        with ns("f1_ag%d" % stream):
            arrive(3, stream, hid1)
        shared.append(share(4 + stream, stream, dot(flat(hid1, stream), down1[...]), par1))
    for load in loads[3:7]:
        load.wait()
    after_first = []
    for stream in range(2):
        with ns("exch1_%d" % stream):
            branch = join(shared[stream], stream, par1)
        kept = (residual[stream] + 0.5 * branch).astype(BF16).astype(F32)
        after_first.append(kept)
        scaled = (kept * gain_mixer_ref[...]).astype(BF16)
        with ns("m_in"):
            put(sma, stream, 0, dot(scaled, wq[...]))
            put(sma, stream, key_cols, dot(scaled, wk[...]))
            put(sma, stream, 2 * key_cols, dot(scaled, extra_weight) + square_lanes(kept))
            scatter(6, stream, sma, rma)
            put(smb, stream, 0, dot(scaled, wv[...]))
            scatter(7, stream, smb, rmb)
            put(smc, stream, 0, dot(scaled, wo[...]))
            scatter(8, stream, smc, rmc)

    with ns("m_rs_a"):
        keys_sum = collect(6, sma, rma)
    extra = keys_sum[:, 2 * key_cols :]
    scale = row_scale(extra)
    for head in range(key_heads):
        for slot, start, factor in (
            (head, head * size, size ** (-0.5)),
            (key_heads + head, key_cols + head * size, 1.0),
        ):
            act = silu(keys_sum[:, start : start + size] * scale)
            unit = act * lax.rsqrt(jnp.sum(act * act, axis=1, keepdims=True) + EPS)
            qk_rows[:, slot, :] = unit * factor
    gates = extra * scale
    beta_pre = gates[:, :heads]
    decay_pre = gates[:, heads : 2 * heads] + bias_ref[...]
    beta_gate = 1.0 / (1.0 + jnp.exp(-beta_pre))
    softplus = jnp.maximum(decay_pre, 0.0) + jnp.log1p(jnp.exp(-jnp.abs(decay_pre)))
    decay_gate = jnp.exp(-decay_exp * softplus)
    for head in range(heads):
        dec_rows[:, head, :] = jnp.broadcast_to(decay_gate[:, head : head + 1], (own_rows, size))

    def look(row, carry):
        pltpu.make_async_copy(state_hbm.at[row], state.at[row], in_sem.at[row]).wait()
        columns = qk_rows[row].T
        for head in range(heads):
            kh = head // repeat
            key_col = columns[:, key_heads + kh : key_heads + kh + 1]
            query_col = columns[:, kh : kh + 1]
            old = state[row, head]
            pred_rows[row, head : head + 1, :] = jnp.sum(old * key_col, axis=0, keepdims=True)
            read_rows[row, head : head + 1, :] = jnp.sum(old * query_col, axis=0, keepdims=True)
        return carry

    with ns("look"):
        lax.fori_loop(0, own_rows, look, 0)

    with ns("m_rs_b"):
        values = silu(collect(7, smb, rmb) * scale)
    with ns("m_rs_c"):
        out_gate = silu(collect(8, smc, rmc) * scale)
    with ns("m_norm"):
        for head in range(heads):
            kh = head // repeat
            cols = slice(head * size, (head + 1) * size)
            decay = decay_gate[:, head : head + 1]
            correction = beta_gate[:, head : head + 1] * (
                values[:, cols] - decay * pred_rows[:, head, :]
            )
            val_rows[:, head, :] = correction
            match = jnp.sum(
                qk_rows[:, kh, :] * qk_rows[:, key_heads + kh, :], axis=1, keepdims=True
            )
            reading = decay * read_rows[:, head, :] + match * correction
            mean = jnp.mean(reading * reading, axis=1, keepdims=True)
            normed = reading * lax.rsqrt(mean + EPS) * head_gain_ref[...]
            nrm[my_s, my_j, :, cols] = (normed * out_gate[:, cols]).astype(BF16)
        spread(9, nrm)

    loads[7].wait()
    shared = []
    for stream in range(2):
        with ns("m_ag%d" % stream):
            arrive(9, stream, nrm)
        shared.append(share(10 + stream, stream, dot(flat(nrm, stream), wout[...]), parm))

    second_bufs = (s2a, r2a, s2b, r2b)
    loads[8].wait()
    loads[9].wait()
    after_mixer = []
    for stream in range(2):
        with ns("exch2_%d" % stream):
            branch = join(shared[stream], stream, parm)
        kept = (after_first[stream] + branch).astype(BF16).astype(F32)
        after_mixer.append(kept)
        with ns("f2_in"):
            ffn_in(12, stream, kept, gain_second_ref, gate2, up2, second_bufs)

    def update(row, carry):
        columns = qk_rows[row].T
        row_dec, row_vals = dec_rows[row], val_rows[row]
        for head in range(heads):
            kh = head // repeat
            key_col = columns[:, key_heads + kh : key_heads + kh + 1]
            state[row, head] = (
                state[row, head] * row_dec[head : head + 1, :]
                + key_col * row_vals[head : head + 1, :]
            )
        return carry

    with ns("update"):
        lax.fori_loop(0, own_rows, update, 0)

    ffn_mid(12, second_bufs, hid2)
    loads[10].wait()
    finals = []
    mine = place_back(depth, piece, tp)
    for stream in range(2):
        with ns("f2_ag%d" % stream):
            arrive(14, stream, hid2)
        product = dot(flat(hid2, stream), down2[...]).astype(BF16)
        for off in range(1, n_tp):
            peer = lax.rem(tp + off, n_tp)
            fin_send[stream, off] = dot(product, place_back(depth, piece, peer)).astype(BF16)
        copies = send_tp(
            15 + stream,
            lambda off: fin_send.at[stream, off],
            lambda off: fin_recv.at[stream, off],
        )
        own_cols = dot(after_mixer[stream].astype(BF16), mine)
        finals.append((copies, own_cols, dot(product, mine)))
    for stream, (copies, own_cols, branch) in enumerate(finals):
        with ns("fin%d" % stream):
            for off in range(1, n_tp):
                copies[off - 1].wait_recv()
                branch = branch + fin_recv[stream, off].astype(F32)
        done = own_cols + 0.5 * branch
        for j in range(half):
            start = start_of(stream, j)
            res_out_ref[start : start + own_rows] = done[j * own_rows : (j + 1) * own_rows].astype(
                BF16
            )

    for copy, stream in pending:
        if stream is None:
            copy.wait_send()
        else:
            pl.when(my_s != stream)(copy.wait_send)


def place_back(rows, cols, peer):
    row = lax.broadcasted_iota(jnp.int32, (rows, cols), 0)
    col = lax.broadcasted_iota(jnp.int32, (rows, cols), 1)
    return jnp.where(row == col + peer * cols, 1.0, 0.0).astype(F32).astype(BF16)


def place_heads(rows, first, lane_start, count):
    row = lax.broadcasted_iota(jnp.int32, (rows, LANES), 0)
    col = lax.broadcasted_iota(jnp.int32, (rows, LANES), 1)
    inside = (col >= lane_start) & (col < lane_start + count)
    hit = inside & (row == col - lane_start + first)
    return jnp.where(hit, 1.0, 0.0).astype(F32).astype(BF16)


def body(
    n_kv,
    n_tp,
    residual_in,
    delta_state,
    norm_gain_first,
    gate_first,
    up_first,
    down_first,
    norm_gain_mixer,
    query_weight,
    key_weight,
    value_weight,
    output_gate_weight,
    beta_weight,
    decay_weight,
    decay_rate,
    decay_bias,
    head_gain,
    out_weight,
    norm_gain_second,
    gate_second,
    up_second,
    down_second,
):
    batch, piece = residual_in.shape
    depth, hidden = gate_first.shape
    own_rows, heads, size, _ = delta_state.shape
    key_cols = query_weight.shape[1]
    val_cols = value_weight.shape[1]
    key_heads = key_cols // size
    hp = pad_lanes(hidden)

    def like(x):
        return pltpu.VMEM(x.shape, x.dtype)

    def slots(cols):
        return pltpu.VMEM((n_kv, own_rows, cols), BF16)

    def split(cols):
        return pltpu.VMEM((2, n_kv // 2, own_rows, cols), BF16)

    def row_buf(count):
        return pltpu.VMEM((own_rows, count, size), F32)

    tp_slots = pltpu.VMEM((2, n_tp, batch // 2, depth), BF16)
    ffn_bufs = [split(hp), slots(hp), split(hp + LANES), slots(hp + LANES), split(hidden), tp_slots]
    wide = 2 * key_cols + LANES
    mixer_bufs = [
        split(wide),
        slots(wide),
        split(val_cols),
        slots(val_cols),
        split(val_cols),
        slots(val_cols),
        split(heads * size),
        tp_slots,
    ]
    big = (
        gate_first,
        up_first,
        down_first,
        query_weight,
        key_weight,
        value_weight,
        output_gate_weight,
        out_weight,
        gate_second,
        up_second,
        down_second,
    )
    small = (
        residual_in,
        norm_gain_first[None, :],
        norm_gain_mixer[None, :],
        norm_gain_second[None, :],
        beta_weight.T,
        decay_weight.T,
        decay_rate[None, :],
        decay_bias[None, :],
        head_gain[None, :],
    )
    vmem = pl.BlockSpec(memory_space=pltpu.VMEM)
    hbm = pl.BlockSpec(memory_space=pl.ANY)
    most = max(n_kv, n_tp)
    return pl.pallas_call(
        functools.partial(kernel, n_kv, n_tp),
        out_shape=(
            pltpu.VMEM(residual_in.shape, BF16),
            pltpu.VMEM(delta_state.shape, F32),
        ),
        in_specs=[vmem] * len(small) + [hbm] * (1 + len(big)),
        out_specs=(vmem, vmem),
        scratch_shapes=[like(x) for x in big]
        + [pltpu.VMEM((n_tp, batch, piece), BF16)]
        + ffn_bufs
        + mixer_bufs
        + ffn_bufs[:-1]
        + [pltpu.VMEM((2, n_tp, batch // 2, piece), BF16)] * 2
        + [row_buf(2 * key_heads), row_buf(heads), row_buf(heads), row_buf(heads), row_buf(heads)]
        + [
            pltpu.SemaphoreType.DMA((len(big),)),
            pltpu.SemaphoreType.DMA((own_rows,)),
            pltpu.SemaphoreType.DMA((17, most)),
            pltpu.SemaphoreType.DMA((17, most)),
        ],
        compiler_params=pltpu.CompilerParams(
            collective_id=0, has_side_effects=True, vmem_limit_bytes=58 * 1024 * 1024
        ),
        name="layer",
    )(*small, delta_state, *big)


def solution(mesh):
    placed = (
        P(None, ("kv", "tp")),
        P("kv", "tp", None, None),
        P("kv"),
        P("kv", "tp"),
        P("kv", "tp"),
        P("tp", "kv"),
        P("kv"),
        P("kv", "tp"),
        P("kv", "tp"),
        P("kv", "tp"),
        P("kv", "tp"),
        P("kv", None),
        P("kv", None),
        P("tp"),
        P("tp"),
        P(),
        P("tp", "kv"),
        P("kv"),
        P("kv", "tp"),
        P("kv", "tp"),
        P("tp", "kv"),
    )
    return jax.shard_map(
        functools.partial(body, mesh.shape["kv"], mesh.shape["tp"]),
        mesh=mesh,
        in_specs=placed,
        out_specs=(P(None, ("kv", "tp")), P("kv", "tp", None, None)),
        check_vma=False,
    )
```

```python
import functools

import jax
import jax.numpy as jnp
from jax import lax
from jax.experimental import pallas as pl
from jax.experimental.pallas import tpu as pltpu
from jax.sharding import PartitionSpec as P

EPS = 1e-06
GROUP = 8
UNROLL = 8
LANES = 128
BF16 = jnp.bfloat16
F32 = jnp.float32
ns = jax.named_scope


def pad_lanes(size):
    return -(-size // LANES) * LANES


def silu(v):
    return v / (1.0 + jnp.exp(-v))


def dot(a, b):
    return jnp.dot(a, b, preferred_element_type=F32)


def dot_first(a, b):
    return lax.dot_general(a, b, (((0,), (0,)), ((), ())), preferred_element_type=F32)


def place(rows, cols, shift):
    row = lax.broadcasted_iota(jnp.int32, (rows, cols), 0)
    col = lax.broadcasted_iota(jnp.int32, (rows, cols), 1)
    return jnp.where(col == row + shift, 1.0, 0.0).astype(F32).astype(BF16)


def kernel(
    n_kv,
    n_tp,
    res_hbm,
    gain_first_hbm,
    gain_mixer_hbm,
    gain_second_hbm,
    beta_hbm,
    decay_hbm,
    rate_hbm,
    bias_hbm,
    head_gain_hbm,
    state_hbm,
    gate1_hbm,
    up1_hbm,
    down1_hbm,
    wq_hbm,
    wk_hbm,
    wv_hbm,
    wo_hbm,
    out_hbm,
    gate2_hbm,
    up2_hbm,
    down2_hbm,
    res_out_ref,
    state,
    res_ref,
    gain_first_ref,
    gain_mixer_ref,
    gain_second_ref,
    beta_ref,
    decay_ref,
    rate_ref,
    bias_ref,
    head_gain_ref,
    gate1,
    up1,
    down1,
    wq,
    wk,
    wv,
    wo,
    wout,
    gate2,
    up2,
    down2,
    res_all,
    s1a,
    r1a,
    s1b,
    r1b,
    hid1,
    par1,
    sma,
    rma,
    smb,
    rmb,
    smc,
    rmc,
    nrm,
    parm,
    s2a,
    r2a,
    s2b,
    r2b,
    hid2,
    fin_send,
    fin_recv,
    qk_rows,
    val_rows,
    dec_rows,
    pred_rows,
    read_rows,
    w_sem,
    small_sem,
    in_sem,
    send_sem,
    recv_sem,
    late_sem,
):
    kv = lax.axis_index("kv")
    tp = lax.axis_index("tp")
    batch, piece = res_ref.shape
    depth = gate1.shape[0]
    width = depth * n_kv
    own_rows = batch // n_kv
    heads = state.shape[1]
    size = state.shape[2]
    key_cols = wq.shape[1]
    key_heads = key_cols // size
    repeat = heads // key_heads
    half = n_kv // 2
    groups = n_kv // GROUP

    turned = lax.rem(kv + GROUP - 2, GROUP)
    my_c = kv // GROUP
    my_s = turned // 4
    my_e = lax.rem(turned, 4) // 2
    my_b = lax.rem(turned, 2)
    my_i = my_c * 4 + my_e * 2 + my_b
    my_j = my_s * half + my_i
    owner = my_s == 0

    def device_at(c, stream, e, b):
        return c * GROUP + lax.rem(stream * 4 + e * 2 + b + 2, GROUP)

    def start_of(stream, j):
        return ((j // 4) * GROUP + (stream * 4 + j % 4 + 2) % GROUP) * own_rows

    def rows_of(value, stream):
        parts = [value[start_of(stream, j) : start_of(stream, j) + own_rows] for j in range(half)]
        return jnp.concatenate(parts, axis=0)

    weight_pairs = (
        (gate1_hbm, gate1),
        (up1_hbm, up1),
        (down1_hbm, down1),
        (wq_hbm, wq),
        (wk_hbm, wk),
        (wv_hbm, wv),
        (wo_hbm, wo),
        (out_hbm, wout),
        (gate2_hbm, gate2),
        (up2_hbm, up2),
        (down2_hbm, down2),
    )
    loads = [
        pltpu.make_async_copy(src, dst, w_sem.at[i]) for i, (src, dst) in enumerate(weight_pairs)
    ]
    small_pairs = (
        (res_hbm, res_ref),
        (gain_first_hbm, gain_first_ref),
        (gain_mixer_hbm, gain_mixer_ref),
        (gain_second_hbm, gain_second_ref),
        (beta_hbm, beta_ref),
        (decay_hbm, decay_ref),
        (rate_hbm, rate_ref),
        (bias_hbm, bias_ref),
        (head_gain_hbm, head_gain_ref),
    )
    smalls = [
        pltpu.make_async_copy(src, dst, small_sem.at[i])
        for i, (src, dst) in enumerate(small_pairs)
    ]
    smalls[0].start()
    barrier = pltpu.get_barrier_semaphore()
    for off in range(1, n_tp):
        pl.semaphore_signal(
            barrier,
            inc=1,
            device_id={"tp": lax.rem(tp + off, n_tp)},
            device_id_type=pl.DeviceIdType.MESH,
        )
    for off in range(1, n_kv):
        pl.semaphore_signal(
            barrier,
            inc=1,
            device_id={"kv": lax.rem(kv + off, n_kv)},
            device_id_type=pl.DeviceIdType.MESH,
        )
    for copy in smalls[1:] + loads[:3]:
        copy.start()
    with ns("barrier"):
        pl.semaphore_wait(barrier, n_tp - 1 + n_kv - 1)

    def remote(src, dst, axis, peer, left, landed):
        return pltpu.make_async_remote_copy(
            src_ref=src,
            dst_ref=dst,
            send_sem=left,
            recv_sem=landed,
            device_id={axis: peer},
            device_id_type=pl.DeviceIdType.MESH,
        )

    sent = []

    def send_tp(event, src_of, dst_of, block):
        sems = send_sem.at[event], recv_sem.at[event]
        for off in range(1, n_tp):
            peer = lax.rem(tp + off, n_tp)
            remote(src_of(off), dst_of(off), "tp", peer, *sems).start()
        every = remote(block, block, "tp", tp, *sems)
        sent.append((None, every))
        return every

    steps = [
        (dc, de, db) for dc in range(groups - 1, -1, -1) for de in (1, 0) for db in (1, 0)
    ]

    def each_kv(stream, make):
        turn = lax.rem(stream + 2 - my_s, 2)
        for dc, de, db in steps:
            c, e, b = lax.rem(my_c + dc, groups), lax.rem(my_e + de, 2), lax.rem(my_b + db, 2)
            last = dc == 0 and de == 0 and db == 0
            copy = make(
                dc * GROUP + turn * 4 + de * 2 + db,
                device_at(c, stream, e, b),
                c * 4 + e * 2 + b,
                last,
            )
            if last:
                pl.when(my_s != stream)(copy.start)
            else:
                copy.start()

    def scatter(event, stream, sends, receives):
        sems = send_sem.at[event], recv_sem.at[event]
        each_kv(
            stream,
            lambda index, peer, j, last: remote(
                sends.at[stream * half + j], receives.at[index], "kv", peer, *sems
            ),
        )

    def collect(event, sends, receives):
        block = receives.at[pl.ds(1, n_kv - 1)]
        every = remote(block, block, "kv", kv, send_sem.at[event], recv_sem.at[event])
        every.wait_recv()
        sent.append((None, every))
        total = sends[my_j].astype(F32)
        for index in range(1, n_kv):
            total = total + receives[index].astype(F32)
        return total

    def spread(event, late, slots):
        own = slots.at[my_j]
        left = send_sem.at[event]
        for stream in range(2):
            each_kv(
                stream,
                lambda index, peer, j, last: remote(
                    own,
                    own,
                    "kv",
                    peer,
                    left,
                    late_sem.at[late + my_s] if last else recv_sem.at[event + my_s],
                ),
            )
        block = slots.at[pl.ds(0, n_kv - 1)]
        sent.append((None, remote(block, block, "kv", kv, left, recv_sem.at[event])))

    def arrive(event, late, stream, slots):
        left = send_sem.at[event]
        block = slots.at[pl.ds(0, half - 1)]
        remote(block, block, "kv", kv, left, recv_sem.at[event + stream]).wait_recv()
        own = slots.at[0]
        pl.when(my_s != stream)(
            remote(own, own, "kv", kv, left, late_sem.at[late + stream]).wait_recv
        )

    def put(ref, stream, offset, value):
        cols = value.shape[1]
        ref[stream * half : (stream + 1) * half, :, offset : offset + cols] = value.reshape(
            half, own_rows, cols
        ).astype(BF16)

    def square_lanes(residual):
        squares = jnp.sum(residual * residual, axis=1, keepdims=True)
        high = squares.astype(BF16).astype(F32)
        lane = lax.broadcasted_iota(jnp.int32, (residual.shape[0], LANES), 1)
        return jnp.where(lane == 64, high, jnp.where(lane == 65, squares - high, 0.0))

    def row_scale(extra):
        squares = extra[:, 64:65] + extra[:, 65:66]
        return lax.rsqrt(squares / width + EPS)

    def flat(slots, stream):
        both = slots[stream * half : (stream + 1) * half].astype(F32)
        return both.reshape(half * own_rows, both.shape[2]).astype(BF16)

    def share(event, stream, value, slots):
        slots[stream, tp] = value.astype(BF16)
        own = slots.at[stream, tp]
        block = slots.at[stream, pl.ds(0, n_tp - 1)]
        return send_tp(event, lambda off: own, lambda off: own, block)

    def join(every, stream, slots):
        every.wait_recv()
        total = slots[stream, 0].astype(F32)
        for other in range(1, n_tp):
            total = total + slots[stream, other].astype(F32)
        return total

    def to_owners(event, stream, sends, receives):
        sems = send_sem.at[event], recv_sem.at[event + stream]
        each_kv(
            0,
            lambda index, peer, j, last: remote(
                sends.at[stream * half + j], receives.at[stream * n_kv + index], "kv", peer, *sems
            ),
        )

    def owned(event, stream, sends, receives):
        block = receives.at[pl.ds(stream * n_kv + 1, n_kv - 1)]
        remote(block, block, "kv", kv, send_sem.at[event], recv_sem.at[event + stream]).wait_recv()
        total = sends[stream * half + my_i].astype(F32)
        for index in range(1, n_kv):
            total = total + receives[stream * n_kv + index].astype(F32)
        return total

    def ffn_in(event, stream, residual, gain_ref, w_gate, w_up, bufs):
        send_a, recv_a, send_b, recv_b = bufs
        up_end = pad_lanes(w_gate.shape[1])
        scaled = (residual * gain_ref[...]).astype(BF16)
        put(send_a, stream, 0, dot(scaled, w_gate[...]))
        to_owners(event, stream, send_a, recv_a)
        put(send_b, stream, 0, dot(scaled, w_up[...]))
        put(send_b, stream, up_end, square_lanes(residual))
        to_owners(event + 2, stream, send_b, recv_b)

    def ffn_mid(event, late, stream, bufs, hid):
        send_a, recv_a, send_b, recv_b = bufs
        hidden_cols = hid.shape[-1]
        up_end = pad_lanes(hidden_cols)
        with ns("f_rs_a"):
            gate_sum = owned(event, stream, send_a, recv_a)[:, :hidden_cols]
        with ns("f_rs_b"):
            rest = owned(event + 2, stream, send_b, recv_b)
        scale = row_scale(rest[:, up_end:])
        hidden = (silu(gate_sum * scale) * (rest[:, :hidden_cols] * scale)).astype(BF16)
        hid[stream * half + my_i] = hidden
        own = hid.at[stream * half + my_i]
        left = send_sem.at[event + 4 + stream]
        for target in range(2):
            for dc, de, db in steps:
                last = dc == 0 and de == 0 and db == 0
                if not (last and target == 0):
                    c, e, b = (
                        lax.rem(my_c + dc, groups),
                        lax.rem(my_e + de, 2),
                        lax.rem(my_b + db, 2),
                    )
                    landed = late_sem.at[late + stream] if last else recv_sem.at[event + 4 + stream]
                    remote(own, own, "kv", device_at(c, target, e, b), left, landed).start()

    def ffn_sent(event, bufs, hid):
        for buf, at in ((bufs[1], event), (bufs[3], event + 2)):
            for cond, count in ((owner, n_kv - 2), (jnp.logical_not(owner), n_kv)):
                block = buf.at[pl.ds(0, count)]
                sent.append(
                    (cond, remote(block, block, "kv", kv, send_sem.at[at], recv_sem.at[at]))
                )
        for stream in range(2):
            block = hid.at[pl.ds(0, n_kv - 1)]
            at = event + 4 + stream
            sent.append((owner, remote(block, block, "kv", kv, send_sem.at[at], recv_sem.at[at])))

    def ffn_arrive(event, late, stream, hid):
        at = event + 4 + stream
        block = hid.at[pl.ds(0, half - 1)]
        remote(block, block, "kv", kv, send_sem.at[at], recv_sem.at[at]).wait_recv()
        own = hid.at[0]
        pl.when(jnp.logical_not(owner))(
            remote(own, own, "kv", kv, send_sem.at[at], late_sem.at[late + stream]).wait_recv
        )

    smalls[0].wait()
    every = send_tp(0, lambda off: res_ref, lambda off: res_all.at[tp], res_all.at[pl.ds(0, n_tp - 1)])
    for load in loads[3:]:
        load.start()
    state_load = pltpu.make_async_copy(state_hbm, state, in_sem)
    state_load.start()
    for copy in smalls[1:]:
        copy.wait()
    decay_exp = jnp.exp(rate_ref[...])
    extra_weight = (
        dot_first(beta_ref[...], place_heads(beta_ref.shape[0], tp * heads, 0, heads))
        + dot_first(decay_ref[...], place_heads(beta_ref.shape[0], tp * heads, heads, heads))
    ).astype(BF16)
    whole = dot(res_ref[...], place(piece, depth, tp * piece))
    with ns("tp_gather"):
        every.wait_recv()
        for off in range(1, n_tp):
            source = lax.rem(tp + n_tp - off, n_tp)
            whole = whole + dot(res_all[source], place(piece, depth, source * piece))

    first_bufs = (s1a, r1a, s1b, r1b)
    residual = [rows_of(whole, stream) for stream in range(2)]
    loads[0].wait()
    loads[1].wait()
    with ns("f1_in"):
        for stream in range(2):
            ffn_in(1, stream, residual[stream], gain_first_ref, gate1, up1, first_bufs)
    for stream in range(2):
        pl.when(owner)(functools.partial(ffn_mid, 1, 0, stream, first_bufs, hid1))
    ffn_sent(1, first_bufs, hid1)
    loads[2].wait()
    shared = []
    for stream in range(2):
        with ns("f1_ag%d" % stream):
            ffn_arrive(1, 0, stream, hid1)
        shared.append(share(7 + stream, stream, dot(flat(hid1, stream), down1[...]), par1))
    for load in loads[3:7]:
        load.wait()
    after_first = []
    for stream in range(2):
        with ns("exch1_%d" % stream):
            branch = join(shared[stream], stream, par1)
        kept = (residual[stream] + 0.5 * branch).astype(BF16).astype(F32)
        after_first.append(kept)
        scaled = (kept * gain_mixer_ref[...]).astype(BF16)
        with ns("m_in"):
            put(sma, stream, 0, dot(scaled, wq[...]))
            put(sma, stream, key_cols, dot(scaled, wk[...]))
            put(sma, stream, 2 * key_cols, dot(scaled, extra_weight) + square_lanes(kept))
            scatter(9, stream, sma, rma)
            put(smb, stream, 0, dot(scaled, wv[...]))
            scatter(10, stream, smb, rmb)
            put(smc, stream, 0, dot(scaled, wo[...]))
            scatter(11, stream, smc, rmc)

    with ns("m_rs_a"):
        keys_sum = collect(9, sma, rma)
    extra = keys_sum[:, 2 * key_cols :]
    scale = row_scale(extra)
    for head in range(key_heads):
        for slot, start, factor in (
            (head, head * size, size ** (-0.5)),
            (key_heads + head, key_cols + head * size, 1.0),
        ):
            act = silu(keys_sum[:, start : start + size] * scale)
            unit = act * lax.rsqrt(jnp.sum(act * act, axis=1, keepdims=True) + EPS)
            qk_rows[:, slot, :] = unit * factor
    gates = extra * scale
    beta_pre = gates[:, :heads]
    decay_pre = gates[:, heads : 2 * heads] + bias_ref[...]
    beta_gate = 1.0 / (1.0 + jnp.exp(-beta_pre))
    softplus = jnp.maximum(decay_pre, 0.0) + jnp.log1p(jnp.exp(-jnp.abs(decay_pre)))
    decay_gate = jnp.exp(-decay_exp * softplus)
    for head in range(heads):
        dec_rows[:, head, :] = jnp.broadcast_to(decay_gate[:, head : head + 1], (own_rows, size))

    def look(row, carry):
        columns = qk_rows[row].T
        for head in range(heads):
            kh = head // repeat
            key_col = columns[:, key_heads + kh : key_heads + kh + 1]
            query_col = columns[:, kh : kh + 1]
            old = state[row, head]
            pred_rows[row, head : head + 1, :] = jnp.sum(old * key_col, axis=0, keepdims=True)
            read_rows[row, head : head + 1, :] = jnp.sum(old * query_col, axis=0, keepdims=True)
        return carry

    with ns("look"):
        state_load.wait()
        lax.fori_loop(0, own_rows, look, 0, unroll=UNROLL)

    with ns("m_rs_b"):
        values = silu(collect(10, smb, rmb) * scale)
    with ns("m_rs_c"):
        out_gate = silu(collect(11, smc, rmc) * scale)
    with ns("m_norm"):
        for head in range(heads):
            kh = head // repeat
            cols = slice(head * size, (head + 1) * size)
            decay = decay_gate[:, head : head + 1]
            correction = beta_gate[:, head : head + 1] * (
                values[:, cols] - decay * pred_rows[:, head, :]
            )
            val_rows[:, head, :] = correction
            match = jnp.sum(
                qk_rows[:, kh, :] * qk_rows[:, key_heads + kh, :], axis=1, keepdims=True
            )
            reading = decay * read_rows[:, head, :] + match * correction
            mean = jnp.mean(reading * reading, axis=1, keepdims=True)
            normed = reading * lax.rsqrt(mean + EPS) * head_gain_ref[...]
            nrm[my_j, :, cols] = (normed * out_gate[:, cols]).astype(BF16)
        spread(12, 2, nrm)

    loads[7].wait()
    shared = []
    for stream in range(2):
        with ns("m_ag%d" % stream):
            arrive(12, 2, stream, nrm)
        shared.append(share(14 + stream, stream, dot(flat(nrm, stream), wout[...]), parm))

    second_bufs = (s2a, r2a, s2b, r2b)
    loads[8].wait()
    loads[9].wait()
    after_mixer = []
    for stream in range(2):
        with ns("exch2_%d" % stream):
            branch = join(shared[stream], stream, parm)
        kept = (after_first[stream] + branch).astype(BF16).astype(F32)
        after_mixer.append(kept)
        with ns("f2_in"):
            ffn_in(16, stream, kept, gain_second_ref, gate2, up2, second_bufs)

    def update(row, carry):
        columns = qk_rows[row].T
        row_dec, row_vals = dec_rows[row], val_rows[row]
        for head in range(heads):
            kh = head // repeat
            key_col = columns[:, key_heads + kh : key_heads + kh + 1]
            state[row, head] = (
                state[row, head] * row_dec[head : head + 1, :]
                + key_col * row_vals[head : head + 1, :]
            )
        return carry

    for stream in range(2):
        pl.when(owner)(functools.partial(ffn_mid, 16, 4, stream, second_bufs, hid2))
    ffn_sent(16, second_bufs, hid2)
    loads[10].wait()
    finals = []
    mine = place_back(depth, piece, tp)
    for stream in range(2):
        with ns("f2_ag%d" % stream):
            ffn_arrive(16, 4, stream, hid2)
        product = dot(flat(hid2, stream), down2[...]).astype(BF16)
        for off in range(1, n_tp):
            peer = lax.rem(tp + off, n_tp)
            fin_send[stream, off] = dot(product, place_back(depth, piece, peer)).astype(BF16)
        every = send_tp(
            22 + stream,
            lambda off: fin_send.at[stream, off],
            lambda off: fin_recv.at[stream, off],
            fin_recv.at[stream, pl.ds(1, n_tp - 1)],
        )
        own_cols = dot(after_mixer[stream].astype(BF16), mine)
        finals.append((every, own_cols, dot(product, mine)))
    with ns("update"):
        lax.fori_loop(0, own_rows, update, 0, unroll=UNROLL)

    for stream, (every, own_cols, branch) in enumerate(finals):
        with ns("fin%d" % stream):
            every.wait_recv()
            for off in range(1, n_tp):
                branch = branch + fin_recv[stream, off].astype(F32)
        done = own_cols + 0.5 * branch
        for j in range(half):
            start = start_of(stream, j)
            res_out_ref[start : start + own_rows] = done[j * own_rows : (j + 1) * own_rows].astype(
                BF16
            )

    for cond, every in sent:
        if cond is None:
            every.wait_send()
        else:
            pl.when(cond)(every.wait_send)


def place_back(rows, cols, peer):
    row = lax.broadcasted_iota(jnp.int32, (rows, cols), 0)
    col = lax.broadcasted_iota(jnp.int32, (rows, cols), 1)
    return jnp.where(row == col + peer * cols, 1.0, 0.0).astype(F32).astype(BF16)


def place_heads(rows, first, lane_start, count):
    row = lax.broadcasted_iota(jnp.int32, (rows, LANES), 0)
    col = lax.broadcasted_iota(jnp.int32, (rows, LANES), 1)
    inside = (col >= lane_start) & (col < lane_start + count)
    hit = inside & (row == col - lane_start + first)
    return jnp.where(hit, 1.0, 0.0).astype(F32).astype(BF16)


def body(
    n_kv,
    n_tp,
    residual_in,
    delta_state,
    norm_gain_first,
    gate_first,
    up_first,
    down_first,
    norm_gain_mixer,
    query_weight,
    key_weight,
    value_weight,
    output_gate_weight,
    beta_weight,
    decay_weight,
    decay_rate,
    decay_bias,
    head_gain,
    out_weight,
    norm_gain_second,
    gate_second,
    up_second,
    down_second,
):
    batch, piece = residual_in.shape
    depth, hidden = gate_first.shape
    own_rows, heads, size, _ = delta_state.shape
    key_cols = query_weight.shape[1]
    val_cols = value_weight.shape[1]
    key_heads = key_cols // size
    hp = pad_lanes(hidden)

    def like(x):
        return pltpu.VMEM(x.shape, x.dtype)

    def slots(cols, times=1):
        return pltpu.VMEM((times * n_kv, own_rows, cols), BF16)


    def row_buf(count):
        return pltpu.VMEM((own_rows, count, size), F32)

    tp_slots = pltpu.VMEM((2, n_tp, batch // 2, depth), BF16)
    ffn_bufs = [
        slots(hp),
        slots(hp, 2),
        slots(hp + LANES),
        slots(hp + LANES, 2),
        slots(hidden),
        tp_slots,
    ]
    wide = 2 * key_cols + LANES
    mixer_bufs = [
        slots(wide),
        slots(wide),
        slots(val_cols),
        slots(val_cols),
        slots(val_cols),
        slots(val_cols),
        slots(heads * size),
        tp_slots,
    ]
    big = (
        gate_first,
        up_first,
        down_first,
        query_weight,
        key_weight,
        value_weight,
        output_gate_weight,
        out_weight,
        gate_second,
        up_second,
        down_second,
    )
    small = (
        residual_in,
        norm_gain_first[None, :],
        norm_gain_mixer[None, :],
        norm_gain_second[None, :],
        beta_weight.T,
        decay_weight.T,
        decay_rate[None, :],
        decay_bias[None, :],
        head_gain[None, :],
    )
    vmem = pl.BlockSpec(memory_space=pltpu.VMEM)
    hbm = pl.BlockSpec(memory_space=pl.ANY)
    return pl.pallas_call(
        functools.partial(kernel, n_kv, n_tp),
        out_shape=(
            pltpu.VMEM(residual_in.shape, BF16),
            pltpu.VMEM(delta_state.shape, F32),
        ),
        in_specs=[hbm] * (len(small) + 1 + len(big)),
        out_specs=(vmem, vmem),
        scratch_shapes=[like(x) for x in (*small, *big)]
        + [pltpu.VMEM((n_tp, batch, piece), BF16)]
        + ffn_bufs
        + mixer_bufs
        + ffn_bufs[:-1]
        + [pltpu.VMEM((2, n_tp, batch // 2, piece), BF16)] * 2
        + [row_buf(2 * key_heads), row_buf(heads), row_buf(heads), row_buf(heads), row_buf(heads)]
        + [
            pltpu.SemaphoreType.DMA((len(big),)),
            pltpu.SemaphoreType.DMA((len(small),)),
            pltpu.SemaphoreType.DMA,
            pltpu.SemaphoreType.DMA((24,)),
            pltpu.SemaphoreType.DMA((24,)),
            pltpu.SemaphoreType.DMA((6,)),
        ],
        compiler_params=pltpu.CompilerParams(
            collective_id=0, has_side_effects=True, vmem_limit_bytes=58 * 1024 * 1024
        ),
        name="layer",
    )(*small, delta_state, *big)


def solution(mesh):
    placed = (
        P(None, ("kv", "tp")),
        P("kv", "tp", None, None),
        P("kv"),
        P("kv", "tp"),
        P("kv", "tp"),
        P("tp", "kv"),
        P("kv"),
        P("kv", "tp"),
        P("kv", "tp"),
        P("kv", "tp"),
        P("kv", "tp"),
        P("kv", None),
        P("kv", None),
        P("tp"),
        P("tp"),
        P(),
        P("tp", "kv"),
        P("kv"),
        P("kv", "tp"),
        P("kv", "tp"),
        P("tp", "kv"),
    )
    return jax.shard_map(
        functools.partial(body, mesh.shape["kv"], mesh.shape["tp"]),
        mesh=mesh,
        in_specs=placed,
        out_specs=(P(None, ("kv", "tp")), P("kv", "tp", None, None)),
        check_vma=False,
    )
```

```python
import functools

import jax
import jax.numpy as jnp
from jax import lax
from jax.experimental import pallas as pl
from jax.experimental.pallas import tpu as pltpu
from jax.sharding import PartitionSpec as P

EPS = 1e-06
GROUP = 8
UNROLL = 8
ORDER = (0, 1)
LANES = 128
BF16 = jnp.bfloat16
F32 = jnp.float32
ns = jax.named_scope


def pad_lanes(size):
    return -(-size // LANES) * LANES


def silu(v):
    return v / (1.0 + jnp.exp(-v))


def dot(a, b):
    return jnp.dot(a, b, preferred_element_type=F32)


def dot_first(a, b):
    return lax.dot_general(a, b, (((0,), (0,)), ((), ())), preferred_element_type=F32)


def place(rows, cols, shift):
    row = lax.broadcasted_iota(jnp.int32, (rows, cols), 0)
    col = lax.broadcasted_iota(jnp.int32, (rows, cols), 1)
    return jnp.where(col == row + shift, 1.0, 0.0).astype(F32).astype(BF16)


def kernel(
    n_kv,
    n_tp,
    res_hbm,
    gain_first_hbm,
    gain_mixer_hbm,
    gain_second_hbm,
    beta_hbm,
    decay_hbm,
    rate_hbm,
    bias_hbm,
    head_gain_hbm,
    state_hbm,
    gate1_hbm,
    up1_hbm,
    down1_hbm,
    wq_hbm,
    wk_hbm,
    wv_hbm,
    wo_hbm,
    out_hbm,
    gate2_hbm,
    up2_hbm,
    down2_hbm,
    res_out_ref,
    state,
    res_ref,
    gain_first_ref,
    gain_mixer_ref,
    gain_second_ref,
    beta_ref,
    decay_ref,
    rate_ref,
    bias_ref,
    head_gain_ref,
    gate1,
    up1,
    down1,
    wq,
    wk,
    wv,
    wo,
    wout,
    gate2,
    up2,
    down2,
    res_all,
    s1a,
    r1a,
    s1b,
    r1b,
    hid1,
    par1,
    sma,
    rma,
    smb,
    rmb,
    smc,
    rmc,
    nrm,
    parm,
    s2a,
    r2a,
    s2b,
    r2b,
    hid2,
    fin_send,
    fin_recv,
    qk_rows,
    val_rows,
    dec_rows,
    pred_rows,
    read_rows,
    w_sem,
    small_sem,
    in_sem,
    send_sem,
    recv_sem,
    late_sem,
):
    kv = lax.axis_index("kv")
    tp = lax.axis_index("tp")
    batch, piece = res_ref.shape
    depth = gate1.shape[0]
    width = depth * n_kv
    own_rows = batch // n_kv
    heads = state.shape[1]
    size = state.shape[2]
    key_cols = wq.shape[1]
    key_heads = key_cols // size
    repeat = heads // key_heads
    half = n_kv // 2
    groups = n_kv // GROUP

    turned = lax.rem(kv + GROUP - 2, GROUP)
    my_c = kv // GROUP
    my_s = turned // 4
    my_e = lax.rem(turned, 4) // 2
    my_b = lax.rem(turned, 2)
    my_i = my_c * 4 + my_e * 2 + my_b
    my_j = my_s * half + my_i
    owner = my_s == 0

    def device_at(c, stream, e, b):
        return c * GROUP + lax.rem(stream * 4 + e * 2 + b + 2, GROUP)

    def start_of(stream, j):
        return ((j // 4) * GROUP + (stream * 4 + j % 4 + 2) % GROUP) * own_rows

    def rows_of(value, stream):
        parts = [value[start_of(stream, j) : start_of(stream, j) + own_rows] for j in range(half)]
        return jnp.concatenate(parts, axis=0)

    weight_pairs = (
        (gate1_hbm, gate1),
        (up1_hbm, up1),
        (down1_hbm, down1),
        (wq_hbm, wq),
        (wk_hbm, wk),
        (wv_hbm, wv),
        (wo_hbm, wo),
        (out_hbm, wout),
        (gate2_hbm, gate2),
        (up2_hbm, up2),
        (down2_hbm, down2),
    )
    loads = [
        pltpu.make_async_copy(src, dst, w_sem.at[i]) for i, (src, dst) in enumerate(weight_pairs)
    ]
    small_pairs = (
        (res_hbm, res_ref),
        (gain_first_hbm, gain_first_ref),
        (gain_mixer_hbm, gain_mixer_ref),
        (gain_second_hbm, gain_second_ref),
        (beta_hbm, beta_ref),
        (decay_hbm, decay_ref),
        (rate_hbm, rate_ref),
        (bias_hbm, bias_ref),
        (head_gain_hbm, head_gain_ref),
    )
    smalls = [
        pltpu.make_async_copy(src, dst, small_sem.at[i])
        for i, (src, dst) in enumerate(small_pairs)
    ]
    smalls[0].start()
    barrier = pltpu.get_barrier_semaphore()
    for off in range(1, n_tp):
        pl.semaphore_signal(
            barrier,
            inc=1,
            device_id={"tp": lax.rem(tp + off, n_tp)},
            device_id_type=pl.DeviceIdType.MESH,
        )

    @pl.when(owner)
    def greet():
        for off in range(1, n_kv):
            pl.semaphore_signal(
                barrier,
                inc=1,
                device_id={"kv": lax.rem(kv + off, n_kv)},
                device_id_type=pl.DeviceIdType.MESH,
            )

    for copy in smalls[1:] + loads[:3]:
        copy.start()
    with ns("barrier"):
        pl.semaphore_wait(barrier, n_tp - 1 + half - 1 + my_s)

    def remote(src, dst, axis, peer, left, landed):
        return pltpu.make_async_remote_copy(
            src_ref=src,
            dst_ref=dst,
            send_sem=left,
            recv_sem=landed,
            device_id={axis: peer},
            device_id_type=pl.DeviceIdType.MESH,
        )

    sent = []

    def send_tp(event, src_of, dst_of, block):
        sems = send_sem.at[event], recv_sem.at[event]
        for off in range(1, n_tp):
            peer = lax.rem(tp + off, n_tp)
            remote(src_of(off), dst_of(off), "tp", peer, *sems).start()
        every = remote(block, block, "tp", tp, *sems)
        sent.append((None, every))
        return every

    steps = [
        (dc, dh, db) for dc in range(groups - 1, -1, -1) for dh in (1, 0) for db in (1, 0)
    ]
    my_h = lax.rem(my_e + my_s, 2)

    def each_kv(stream, make):
        turn = lax.rem(stream + 2 - my_s, 2)
        for dc, dh, db in steps:
            c, b = lax.rem(my_c + dc, groups), lax.rem(my_b + db, 2)
            e = lax.rem(my_h + dh + stream, 2)
            last = dc == 0 and dh == 0 and db == 0
            copy = make(
                dc * GROUP + turn * 4 + dh * 2 + db,
                device_at(c, stream, e, b),
                c * 4 + e * 2 + b,
                last,
            )
            if last:
                pl.when(my_s != stream)(copy.start)
            else:
                copy.start()

    def scatter(event, stream, sends, receives):
        sems = send_sem.at[event], recv_sem.at[event]
        each_kv(
            stream,
            lambda index, peer, j, last: remote(
                sends.at[stream * half + j], receives.at[index], "kv", peer, *sems
            ),
        )

    def collect(event, sends, receives):
        block = receives.at[pl.ds(1, n_kv - 1)]
        every = remote(block, block, "kv", kv, send_sem.at[event], recv_sem.at[event])
        every.wait_recv()
        sent.append((None, every))
        total = sends[my_j].astype(F32)
        for index in range(1, n_kv):
            total = total + receives[index].astype(F32)
        return total

    def spread(event, late, slots):
        own = slots.at[my_j]
        left = send_sem.at[event]
        for stream in range(2):
            each_kv(
                stream,
                lambda index, peer, j, last: remote(
                    own,
                    own,
                    "kv",
                    peer,
                    left,
                    late_sem.at[late + my_s] if last else recv_sem.at[event + my_s],
                ),
            )
        block = slots.at[pl.ds(0, n_kv - 1)]
        sent.append((None, remote(block, block, "kv", kv, left, recv_sem.at[event])))

    def arrive(event, late, stream, slots):
        left = send_sem.at[event]
        block = slots.at[pl.ds(0, half - 1)]
        remote(block, block, "kv", kv, left, recv_sem.at[event + stream]).wait_recv()
        own = slots.at[0]
        pl.when(my_s != stream)(
            remote(own, own, "kv", kv, left, late_sem.at[late + stream]).wait_recv
        )

    def put(ref, stream, offset, value):
        cols = value.shape[1]
        ref[stream * half : (stream + 1) * half, :, offset : offset + cols] = value.reshape(
            half, own_rows, cols
        ).astype(BF16)

    def square_lanes(residual):
        squares = jnp.sum(residual * residual, axis=1, keepdims=True)
        high = squares.astype(BF16).astype(F32)
        lane = lax.broadcasted_iota(jnp.int32, (residual.shape[0], LANES), 1)
        return jnp.where(lane == 64, high, jnp.where(lane == 65, squares - high, 0.0))

    def row_scale(extra):
        squares = extra[:, 64:65] + extra[:, 65:66]
        return lax.rsqrt(squares / width + EPS)

    def flat(slots, stream):
        both = slots[stream * half : (stream + 1) * half].astype(F32)
        return both.reshape(half * own_rows, both.shape[2]).astype(BF16)

    def share(event, stream, value, slots):
        slots[stream, tp] = value.astype(BF16)
        own = slots.at[stream, tp]
        block = slots.at[stream, pl.ds(0, n_tp - 1)]
        return send_tp(event, lambda off: own, lambda off: own, block)

    def join(every, stream, slots):
        every.wait_recv()
        total = slots[stream, 0].astype(F32)
        for other in range(1, n_tp):
            total = total + slots[stream, other].astype(F32)
        return total

    def to_owners(event, stream, sends, receives):
        sems = send_sem.at[event], recv_sem.at[event + stream]
        each_kv(
            0,
            lambda index, peer, j, last: remote(
                sends.at[stream * half + j], receives.at[stream * n_kv + index], "kv", peer, *sems
            ),
        )

    def owned(event, stream, sends, receives):
        block = receives.at[pl.ds(stream * n_kv + 1, n_kv - 1)]
        remote(block, block, "kv", kv, send_sem.at[event], recv_sem.at[event + stream]).wait_recv()
        total = sends[stream * half + my_i].astype(F32)
        for index in range(1, n_kv):
            total = total + receives[stream * n_kv + index].astype(F32)
        return total

    def ffn_in(event, stream, residual, gain_ref, w_gate, w_up, bufs):
        send_a, recv_a, send_b, recv_b = bufs
        up_end = pad_lanes(w_gate.shape[1])
        scaled = (residual * gain_ref[...]).astype(BF16)
        put(send_a, stream, 0, dot(scaled, w_gate[...]))
        to_owners(event, stream, send_a, recv_a)
        put(send_b, stream, 0, dot(scaled, w_up[...]))
        put(send_b, stream, up_end, square_lanes(residual))
        to_owners(event + 2, stream, send_b, recv_b)

    def ffn_mid(event, late, stream, bufs, hid):
        send_a, recv_a, send_b, recv_b = bufs
        hidden_cols = hid.shape[-1]
        up_end = pad_lanes(hidden_cols)
        with ns("f_rs_a"):
            gate_sum = owned(event, stream, send_a, recv_a)[:, :hidden_cols]
        with ns("f_rs_b"):
            rest = owned(event + 2, stream, send_b, recv_b)
        scale = row_scale(rest[:, up_end:])
        hidden = (silu(gate_sum * scale) * (rest[:, :hidden_cols] * scale)).astype(BF16)
        hid[stream * half + my_i] = hidden
        own = hid.at[stream * half + my_i]
        left = send_sem.at[event + 4 + stream]
        for target in range(2):
            for dc, dh, db in steps:
                last = dc == 0 and dh == 0 and db == 0
                if not (last and target == 0):
                    c, e, b = (
                        lax.rem(my_c + dc, groups),
                        lax.rem(my_h + dh + target, 2),
                        lax.rem(my_b + db, 2),
                    )
                    landed = late_sem.at[late + stream] if last else recv_sem.at[event + 4 + stream]
                    remote(own, own, "kv", device_at(c, target, e, b), left, landed).start()

    def ffn_sent(event, bufs, hid):
        for buf, at in ((bufs[1], event), (bufs[3], event + 2)):
            for cond, count in ((owner, n_kv - 2), (jnp.logical_not(owner), n_kv)):
                block = buf.at[pl.ds(0, count)]
                sent.append(
                    (cond, remote(block, block, "kv", kv, send_sem.at[at], recv_sem.at[at]))
                )
        for stream in range(2):
            block = hid.at[pl.ds(0, n_kv - 1)]
            at = event + 4 + stream
            sent.append((owner, remote(block, block, "kv", kv, send_sem.at[at], recv_sem.at[at])))

    def ffn_arrive(event, late, stream, hid):
        at = event + 4 + stream
        block = hid.at[pl.ds(0, half - 1)]
        remote(block, block, "kv", kv, send_sem.at[at], recv_sem.at[at]).wait_recv()
        own = hid.at[0]
        pl.when(jnp.logical_not(owner))(
            remote(own, own, "kv", kv, send_sem.at[at], late_sem.at[late + stream]).wait_recv
        )

    smalls[0].wait()
    every = send_tp(0, lambda off: res_ref, lambda off: res_all.at[tp], res_all.at[pl.ds(0, n_tp - 1)])
    for load in loads[3:]:
        load.start()
    state_load = pltpu.make_async_copy(state_hbm, state, in_sem)
    state_load.start()
    for copy in smalls[1:]:
        copy.wait()
    decay_exp = jnp.exp(rate_ref[...])
    extra_weight = (
        dot_first(beta_ref[...], place_heads(beta_ref.shape[0], tp * heads, 0, heads))
        + dot_first(decay_ref[...], place_heads(beta_ref.shape[0], tp * heads, heads, heads))
    ).astype(BF16)
    whole = dot(res_ref[...], place(piece, depth, tp * piece))
    with ns("tp_gather"):
        every.wait_recv()
        for off in range(1, n_tp):
            source = lax.rem(tp + n_tp - off, n_tp)
            whole = whole + dot(res_all[source], place(piece, depth, source * piece))

    first_bufs = (s1a, r1a, s1b, r1b)
    residual = [rows_of(whole, stream) for stream in range(2)]
    loads[0].wait()
    loads[1].wait()
    with ns("f1_in"):
        for stream in ORDER:
            ffn_in(1, stream, residual[stream], gain_first_ref, gate1, up1, first_bufs)
    for stream in ORDER:
        pl.when(owner)(functools.partial(ffn_mid, 1, 0, stream, first_bufs, hid1))
    ffn_sent(1, first_bufs, hid1)
    def first_out(stream):
        with ns("f1_ag%d" % stream):
            ffn_arrive(1, 0, stream, hid1)
        return share(7 + stream, stream, dot(flat(hid1, stream), down1[...]), par1)

    after_first = [None, None]

    def mixer_in(stream, shared):
        with ns("exch1_%d" % stream):
            branch = join(shared, stream, par1)
        kept = (residual[stream] + 0.5 * branch).astype(BF16).astype(F32)
        after_first[stream] = kept
        scaled = (kept * gain_mixer_ref[...]).astype(BF16)
        with ns("m_in"):
            put(sma, stream, 0, dot(scaled, wq[...]))
            put(sma, stream, key_cols, dot(scaled, wk[...]))
            put(sma, stream, 2 * key_cols, dot(scaled, extra_weight) + square_lanes(kept))
            scatter(9, stream, sma, rma)
            put(smb, stream, 0, dot(scaled, wv[...]))
            scatter(10, stream, smb, rmb)
            put(smc, stream, 0, dot(scaled, wo[...]))
            scatter(11, stream, smc, rmc)

    for load in loads[2:7]:
        load.wait()
    shared = first_out(ORDER[0])
    later = first_out(ORDER[1])
    mixer_in(ORDER[0], shared)
    mixer_in(ORDER[1], later)

    with ns("m_rs_a"):
        keys_sum = collect(9, sma, rma)
    extra = keys_sum[:, 2 * key_cols :]
    scale = row_scale(extra)
    for head in range(key_heads):
        for slot, start, factor in (
            (head, head * size, size ** (-0.5)),
            (key_heads + head, key_cols + head * size, 1.0),
        ):
            act = silu(keys_sum[:, start : start + size] * scale)
            unit = act * lax.rsqrt(jnp.sum(act * act, axis=1, keepdims=True) + EPS)
            qk_rows[:, slot, :] = unit * factor
    gates = extra * scale
    beta_pre = gates[:, :heads]
    decay_pre = gates[:, heads : 2 * heads] + bias_ref[...]
    beta_gate = 1.0 / (1.0 + jnp.exp(-beta_pre))
    softplus = jnp.maximum(decay_pre, 0.0) + jnp.log1p(jnp.exp(-jnp.abs(decay_pre)))
    decay_gate = jnp.exp(-decay_exp * softplus)
    for head in range(heads):
        dec_rows[:, head, :] = jnp.broadcast_to(decay_gate[:, head : head + 1], (own_rows, size))

    def look(row, carry):
        columns = qk_rows[row].T
        for head in range(heads):
            kh = head // repeat
            key_col = columns[:, key_heads + kh : key_heads + kh + 1]
            query_col = columns[:, kh : kh + 1]
            old = state[row, head]
            pred_rows[row, head : head + 1, :] = jnp.sum(old * key_col, axis=0, keepdims=True)
            read_rows[row, head : head + 1, :] = jnp.sum(old * query_col, axis=0, keepdims=True)
        return carry

    with ns("look"):
        state_load.wait()
        lax.fori_loop(0, own_rows, look, 0, unroll=UNROLL)

    with ns("m_rs_b"):
        values = silu(collect(10, smb, rmb) * scale)
    with ns("m_rs_c"):
        out_gate = silu(collect(11, smc, rmc) * scale)
    with ns("m_norm"):
        for head in range(heads):
            kh = head // repeat
            cols = slice(head * size, (head + 1) * size)
            decay = decay_gate[:, head : head + 1]
            correction = beta_gate[:, head : head + 1] * (
                values[:, cols] - decay * pred_rows[:, head, :]
            )
            val_rows[:, head, :] = correction
            match = jnp.sum(
                qk_rows[:, kh, :] * qk_rows[:, key_heads + kh, :], axis=1, keepdims=True
            )
            reading = decay * read_rows[:, head, :] + match * correction
            mean = jnp.mean(reading * reading, axis=1, keepdims=True)
            normed = reading * lax.rsqrt(mean + EPS) * head_gain_ref[...]
            nrm[my_j, :, cols] = (normed * out_gate[:, cols]).astype(BF16)
        spread(12, 2, nrm)

    def mixer_out(stream):
        with ns("m_ag%d" % stream):
            arrive(12, 2, stream, nrm)
        return share(14 + stream, stream, dot(flat(nrm, stream), wout[...]), parm)

    second_bufs = (s2a, r2a, s2b, r2b)
    after_mixer = [None, None]

    def second_in(stream, shared):
        with ns("exch2_%d" % stream):
            branch = join(shared, stream, parm)
        kept = (after_first[stream] + branch).astype(BF16).astype(F32)
        after_mixer[stream] = kept
        with ns("f2_in"):
            ffn_in(16, stream, kept, gain_second_ref, gate2, up2, second_bufs)

    for load in loads[7:10]:
        load.wait()
    shared = mixer_out(ORDER[0])
    second_in(ORDER[0], shared)
    second_in(ORDER[1], mixer_out(ORDER[1]))

    def update(row, carry):
        columns = qk_rows[row].T
        row_dec, row_vals = dec_rows[row], val_rows[row]
        for head in range(heads):
            kh = head // repeat
            key_col = columns[:, key_heads + kh : key_heads + kh + 1]
            state[row, head] = (
                state[row, head] * row_dec[head : head + 1, :]
                + key_col * row_vals[head : head + 1, :]
            )
        return carry

    for stream in ORDER:
        pl.when(owner)(functools.partial(ffn_mid, 16, 4, stream, second_bufs, hid2))
    ffn_sent(16, second_bufs, hid2)
    loads[10].wait()
    finals = []
    mine = place_back(depth, piece, tp)
    for stream in ORDER:
        with ns("f2_ag%d" % stream):
            ffn_arrive(16, 4, stream, hid2)
        product = dot(flat(hid2, stream), down2[...]).astype(BF16)
        for off in range(1, n_tp):
            peer = lax.rem(tp + off, n_tp)
            fin_send[stream, off] = dot(product, place_back(depth, piece, peer)).astype(BF16)
        every = send_tp(
            22 + stream,
            lambda off: fin_send.at[stream, off],
            lambda off: fin_recv.at[stream, off],
            fin_recv.at[stream, pl.ds(1, n_tp - 1)],
        )
        own_cols = dot(after_mixer[stream].astype(BF16), mine)
        finals.append((stream, every, own_cols, dot(product, mine)))
    with ns("update"):
        lax.fori_loop(0, own_rows, update, 0, unroll=UNROLL)

    for stream, every, own_cols, branch in finals:
        with ns("fin%d" % stream):
            every.wait_recv()
            for off in range(1, n_tp):
                branch = branch + fin_recv[stream, off].astype(F32)
        done = own_cols + 0.5 * branch
        for j in range(half):
            start = start_of(stream, j)
            res_out_ref[start : start + own_rows] = done[j * own_rows : (j + 1) * own_rows].astype(
                BF16
            )

    for cond, every in sent:
        if cond is None:
            every.wait_send()
        else:
            pl.when(cond)(every.wait_send)


def finish(res_ref, state_ref, res_out, state_out, sem):
    rows = state_ref.shape[0]
    copies = [
        pltpu.make_async_copy(state_ref.at[row], state_out.at[row], sem.at[row])
        for row in range(rows)
    ]
    copies.append(pltpu.make_async_copy(res_ref, res_out, sem.at[rows]))
    for copy in copies:
        copy.start()
    for copy in copies:
        copy.wait()


def place_back(rows, cols, peer):
    row = lax.broadcasted_iota(jnp.int32, (rows, cols), 0)
    col = lax.broadcasted_iota(jnp.int32, (rows, cols), 1)
    return jnp.where(row == col + peer * cols, 1.0, 0.0).astype(F32).astype(BF16)


def place_heads(rows, first, lane_start, count):
    row = lax.broadcasted_iota(jnp.int32, (rows, LANES), 0)
    col = lax.broadcasted_iota(jnp.int32, (rows, LANES), 1)
    inside = (col >= lane_start) & (col < lane_start + count)
    hit = inside & (row == col - lane_start + first)
    return jnp.where(hit, 1.0, 0.0).astype(F32).astype(BF16)


def body(
    n_kv,
    n_tp,
    residual_in,
    delta_state,
    norm_gain_first,
    gate_first,
    up_first,
    down_first,
    norm_gain_mixer,
    query_weight,
    key_weight,
    value_weight,
    output_gate_weight,
    beta_weight,
    decay_weight,
    decay_rate,
    decay_bias,
    head_gain,
    out_weight,
    norm_gain_second,
    gate_second,
    up_second,
    down_second,
):
    batch, piece = residual_in.shape
    depth, hidden = gate_first.shape
    own_rows, heads, size, _ = delta_state.shape
    key_cols = query_weight.shape[1]
    val_cols = value_weight.shape[1]
    key_heads = key_cols // size
    hp = pad_lanes(hidden)

    def like(x):
        return pltpu.VMEM(x.shape, x.dtype)

    def slots(cols, times=1):
        return pltpu.VMEM((times * n_kv, own_rows, cols), BF16)


    def row_buf(count):
        return pltpu.VMEM((own_rows, count, size), F32)

    tp_slots = pltpu.VMEM((2, n_tp, batch // 2, depth), BF16)
    ffn_bufs = [
        slots(hp),
        slots(hp, 2),
        slots(hp + LANES),
        slots(hp + LANES, 2),
        slots(hidden),
        tp_slots,
    ]
    wide = 2 * key_cols + LANES
    mixer_bufs = [
        slots(wide),
        slots(wide),
        slots(val_cols),
        slots(val_cols),
        slots(val_cols),
        slots(val_cols),
        slots(heads * size),
        tp_slots,
    ]
    big = (
        gate_first,
        up_first,
        down_first,
        query_weight,
        key_weight,
        value_weight,
        output_gate_weight,
        out_weight,
        gate_second,
        up_second,
        down_second,
    )
    small = (
        residual_in,
        norm_gain_first[None, :],
        norm_gain_mixer[None, :],
        norm_gain_second[None, :],
        beta_weight.T,
        decay_weight.T,
        decay_rate[None, :],
        decay_bias[None, :],
        head_gain[None, :],
    )
    vmem = pl.BlockSpec(memory_space=pltpu.VMEM)
    hbm = pl.BlockSpec(memory_space=pl.ANY)
    done = pl.pallas_call(
        functools.partial(kernel, n_kv, n_tp),
        out_shape=(
            pltpu.VMEM(residual_in.shape, BF16),
            pltpu.VMEM(delta_state.shape, F32),
        ),
        in_specs=[hbm] * (len(small) + 1 + len(big)),
        out_specs=(vmem, vmem),
        scratch_shapes=[like(x) for x in (*small, *big)]
        + [pltpu.VMEM((n_tp, batch, piece), BF16)]
        + ffn_bufs
        + mixer_bufs
        + ffn_bufs[:-1]
        + [pltpu.VMEM((2, n_tp, batch // 2, piece), BF16)] * 2
        + [row_buf(2 * key_heads), row_buf(heads), row_buf(heads), row_buf(heads), row_buf(heads)]
        + [
            pltpu.SemaphoreType.DMA((len(big),)),
            pltpu.SemaphoreType.DMA((len(small),)),
            pltpu.SemaphoreType.DMA,
            pltpu.SemaphoreType.DMA((24,)),
            pltpu.SemaphoreType.DMA((24,)),
            pltpu.SemaphoreType.DMA((6,)),
        ],
        compiler_params=pltpu.CompilerParams(
            collective_id=0, has_side_effects=True, vmem_limit_bytes=58 * 1024 * 1024
        ),
        name="layer",
    )(*small, delta_state, *big)
    return pl.pallas_call(
        finish,
        out_shape=(
            jax.ShapeDtypeStruct(residual_in.shape, BF16),
            jax.ShapeDtypeStruct(delta_state.shape, F32),
        ),
        in_specs=[vmem, vmem],
        out_specs=(hbm, hbm),
        scratch_shapes=[pltpu.SemaphoreType.DMA((own_rows + 1,))],
        compiler_params=pltpu.CompilerParams(vmem_limit_bytes=1024 * 1024),
        name="finish",
    )(*done)


def solution(mesh):
    placed = (
        P(None, ("kv", "tp")),
        P("kv", "tp", None, None),
        P("kv"),
        P("kv", "tp"),
        P("kv", "tp"),
        P("tp", "kv"),
        P("kv"),
        P("kv", "tp"),
        P("kv", "tp"),
        P("kv", "tp"),
        P("kv", "tp"),
        P("kv", None),
        P("kv", None),
        P("tp"),
        P("tp"),
        P(),
        P("tp", "kv"),
        P("kv"),
        P("kv", "tp"),
        P("kv", "tp"),
        P("tp", "kv"),
    )
    return jax.shard_map(
        functools.partial(body, mesh.shape["kv"], mesh.shape["tp"]),
        mesh=mesh,
        in_specs=placed,
        out_specs=(P(None, ("kv", "tp")), P("kv", "tp", None, None)),
        check_vma=False,
    )
```

```python
import functools

import jax
import jax.numpy as jnp
from jax import lax
from jax.experimental import pallas as pl
from jax.experimental.pallas import tpu as pltpu
from jax.sharding import PartitionSpec as P

EPS = 1e-06
GROUP = 8
UNROLL = 8
ORDER = (0, 1)
LANES = 128
BF16 = jnp.bfloat16
F32 = jnp.float32
ns = jax.named_scope


def pad_lanes(size):
    return -(-size // LANES) * LANES


def silu(v):
    return v / (1.0 + jnp.exp(-v))


def dot(a, b):
    return jnp.dot(a, b, preferred_element_type=F32)


def dot_first(a, b):
    return lax.dot_general(a, b, (((0,), (0,)), ((), ())), preferred_element_type=F32)


def kernel(
    n_kv,
    n_tp,
    res_hbm,
    gain_first_hbm,
    gain_mixer_hbm,
    gain_second_hbm,
    beta_hbm,
    decay_hbm,
    rate_hbm,
    bias_hbm,
    head_gain_hbm,
    state_hbm,
    gate1_hbm,
    up1_hbm,
    down1_hbm,
    wq_hbm,
    wk_hbm,
    wv_hbm,
    wo_hbm,
    out_hbm,
    gate2_hbm,
    up2_hbm,
    down2_hbm,
    res_out_ref,
    state,
    gain_first_ref,
    gain_mixer_ref,
    gain_second_ref,
    beta_ref,
    decay_ref,
    rate_ref,
    bias_ref,
    head_gain_ref,
    gate1,
    up1,
    down1,
    wq,
    wk,
    wv,
    wo,
    wout,
    gate2,
    up2,
    down2,
    res_all,
    s1a,
    r1a,
    s1b,
    r1b,
    hid1,
    par1,
    sma,
    rma,
    smb,
    rmb,
    smc,
    rmc,
    nrm,
    parm,
    s2a,
    r2a,
    s2b,
    r2b,
    hid2,
    kept_rows,
    product,
    fin_recv,
    qk_rows,
    val_rows,
    dec_rows,
    pred_rows,
    read_rows,
    w_sem,
    small_sem,
    in_sem,
    send_sem,
    recv_sem,
    late_sem,
):
    kv = lax.axis_index("kv")
    tp = lax.axis_index("tp")
    _, batch, piece = res_all.shape
    depth = gate1.shape[0]
    width = depth * n_kv
    own_rows = batch // n_kv
    heads = state.shape[1]
    size = state.shape[2]
    key_cols = wq.shape[1]
    key_heads = key_cols // size
    repeat = heads // key_heads
    half = n_kv // 2
    groups = n_kv // GROUP

    turned = lax.rem(kv + GROUP - 2, GROUP)
    my_c = kv // GROUP
    my_s = turned // 4
    my_e = lax.rem(turned, 4) // 2
    my_b = lax.rem(turned, 2)
    my_i = my_c * 4 + my_e * 2 + my_b
    my_j = my_s * half + my_i
    owner = my_s == 0

    def device_at(c, stream, e, b):
        return c * GROUP + lax.rem(stream * 4 + e * 2 + b + 2, GROUP)

    def start_of(stream, j):
        return ((j // 4) * GROUP + (stream * 4 + j % 4 + 2) % GROUP) * own_rows

    def rows_of(value, stream):
        parts = [value[start_of(stream, j) : start_of(stream, j) + own_rows] for j in range(half)]
        return jnp.concatenate(parts, axis=0)

    weight_pairs = (
        (gate1_hbm, gate1),
        (up1_hbm, up1),
        (down1_hbm, down1),
        (wq_hbm, wq),
        (wk_hbm, wk),
        (wv_hbm, wv),
        (wo_hbm, wo),
        (out_hbm, wout),
        (gate2_hbm, gate2),
        (up2_hbm, up2),
        (down2_hbm, down2),
    )
    loads = [
        pltpu.make_async_copy(src, dst, w_sem.at[i]) for i, (src, dst) in enumerate(weight_pairs)
    ]
    small_pairs = (
        (res_hbm, res_all.at[tp]),
        (gain_first_hbm, gain_first_ref),
        (gain_mixer_hbm, gain_mixer_ref),
        (gain_second_hbm, gain_second_ref),
        (beta_hbm, beta_ref),
        (decay_hbm, decay_ref),
        (rate_hbm, rate_ref),
        (bias_hbm, bias_ref),
        (head_gain_hbm, head_gain_ref),
    )
    smalls = [
        pltpu.make_async_copy(src, dst, small_sem.at[i])
        for i, (src, dst) in enumerate(small_pairs)
    ]
    smalls[0].start()
    barrier = pltpu.get_barrier_semaphore()
    for off in range(1, n_tp):
        pl.semaphore_signal(
            barrier,
            inc=1,
            device_id={"tp": lax.rem(tp + off, n_tp)},
            device_id_type=pl.DeviceIdType.MESH,
        )

    @pl.when(owner)
    def greet():
        for off in range(1, n_kv):
            pl.semaphore_signal(
                barrier,
                inc=1,
                device_id={"kv": lax.rem(kv + off, n_kv)},
                device_id_type=pl.DeviceIdType.MESH,
            )

    for copy in smalls[1:] + loads[:3]:
        copy.start()
    with ns("barrier"):
        pl.semaphore_wait(barrier, n_tp - 1 + half - 1 + my_s)

    def remote(src, dst, axis, peer, left, landed):
        return pltpu.make_async_remote_copy(
            src_ref=src,
            dst_ref=dst,
            send_sem=left,
            recv_sem=landed,
            device_id={axis: peer},
            device_id_type=pl.DeviceIdType.MESH,
        )

    sent = []

    def send_tp(event, src_of, dst_of, block):
        sems = send_sem.at[event], recv_sem.at[event]
        for off in range(1, n_tp):
            peer = lax.rem(tp + off, n_tp)
            remote(src_of(off), dst_of(off), "tp", peer, *sems).start()
        every = remote(block, block, "tp", tp, *sems)
        sent.append((None, every))
        return every

    steps = [
        (dc, dh, db) for dc in range(groups - 1, -1, -1) for dh in (1, 0) for db in (1, 0)
    ]
    my_h = lax.rem(my_e + my_s, 2)

    def each_kv(stream, make):
        turn = lax.rem(stream + 2 - my_s, 2)
        for dc, dh, db in steps:
            c, b = lax.rem(my_c + dc, groups), lax.rem(my_b + db, 2)
            e = lax.rem(my_h + dh + stream, 2)
            last = dc == 0 and dh == 0 and db == 0
            copy = make(
                dc * GROUP + turn * 4 + dh * 2 + db,
                device_at(c, stream, e, b),
                c * 4 + e * 2 + b,
                last,
            )
            if last:
                pl.when(my_s != stream)(copy.start)
            else:
                copy.start()

    def scatter(event, stream, sends, receives):
        sems = send_sem.at[event], recv_sem.at[event]
        each_kv(
            stream,
            lambda index, peer, j, last: remote(
                sends.at[stream * half + j], receives.at[index], "kv", peer, *sems
            ),
        )

    def collect(event, sends, receives):
        block = receives.at[pl.ds(1, n_kv - 1)]
        every = remote(block, block, "kv", kv, send_sem.at[event], recv_sem.at[event])
        every.wait_recv()
        sent.append((None, every))
        total = sends[my_j].astype(F32)
        for index in range(1, n_kv):
            total = total + receives[index].astype(F32)
        return total

    def spread(event, late, slots):
        own = slots.at[my_j]
        left = send_sem.at[event]
        for stream in range(2):
            each_kv(
                stream,
                lambda index, peer, j, last: remote(
                    own,
                    own,
                    "kv",
                    peer,
                    left,
                    late_sem.at[late + my_s] if last else recv_sem.at[event + my_s],
                ),
            )
        block = slots.at[pl.ds(0, n_kv - 1)]
        sent.append((None, remote(block, block, "kv", kv, left, recv_sem.at[event])))

    def arrive(event, late, stream, slots):
        left = send_sem.at[event]
        block = slots.at[pl.ds(0, half - 1)]
        remote(block, block, "kv", kv, left, recv_sem.at[event + stream]).wait_recv()
        own = slots.at[0]
        pl.when(my_s != stream)(
            remote(own, own, "kv", kv, left, late_sem.at[late + stream]).wait_recv
        )

    def put(ref, stream, offset, value):
        cols = value.shape[1]
        ref[stream * half : (stream + 1) * half, :, offset : offset + cols] = value.reshape(
            half, own_rows, cols
        ).astype(BF16)

    def square_lanes(residual):
        squares = jnp.sum(residual * residual, axis=1, keepdims=True)
        high = squares.astype(BF16).astype(F32)
        lane = lax.broadcasted_iota(jnp.int32, (residual.shape[0], LANES), 1)
        return jnp.where(lane == 64, high, jnp.where(lane == 65, squares - high, 0.0))

    def row_scale(extra):
        squares = extra[:, 64:65] + extra[:, 65:66]
        return lax.rsqrt(squares / width + EPS)

    def flat(slots, stream):
        both = slots[stream * half : (stream + 1) * half].astype(F32)
        return both.reshape(half * own_rows, both.shape[2]).astype(BF16)

    def share(event, stream, value, slots):
        slots[stream, tp] = value.astype(BF16)
        own = slots.at[stream, tp]
        block = slots.at[stream, pl.ds(0, n_tp - 1)]
        return send_tp(event, lambda off: own, lambda off: own, block)

    def join(every, stream, slots):
        every.wait_recv()
        total = slots[stream, 0].astype(F32)
        for other in range(1, n_tp):
            total = total + slots[stream, other].astype(F32)
        return total

    def to_owners(event, stream, sends, receives):
        sems = send_sem.at[event], recv_sem.at[event + stream]
        each_kv(
            0,
            lambda index, peer, j, last: remote(
                sends.at[stream * half + j], receives.at[stream * n_kv + index], "kv", peer, *sems
            ),
        )

    def owned(event, stream, sends, receives):
        block = receives.at[pl.ds(stream * n_kv + 1, n_kv - 1)]
        remote(block, block, "kv", kv, send_sem.at[event], recv_sem.at[event + stream]).wait_recv()
        total = sends[stream * half + my_i].astype(F32)
        for index in range(1, n_kv):
            total = total + receives[stream * n_kv + index].astype(F32)
        return total

    def ffn_in(event, stream, residual, gain_ref, w_gate, w_up, bufs):
        send_a, recv_a, send_b, recv_b = bufs
        up_end = pad_lanes(w_gate.shape[1])
        scaled = (residual * gain_ref[...]).astype(BF16)
        put(send_a, stream, 0, dot(scaled, w_gate[...]))
        to_owners(event, stream, send_a, recv_a)
        put(send_b, stream, 0, dot(scaled, w_up[...]))
        put(send_b, stream, up_end, square_lanes(residual))
        to_owners(event + 2, stream, send_b, recv_b)

    def ffn_mid(event, late, stream, bufs, hid):
        send_a, recv_a, send_b, recv_b = bufs
        hidden_cols = hid.shape[-1]
        up_end = pad_lanes(hidden_cols)
        with ns("f_rs_a"):
            gate_sum = owned(event, stream, send_a, recv_a)[:, :hidden_cols]
        with ns("f_rs_b"):
            rest = owned(event + 2, stream, send_b, recv_b)
        scale = row_scale(rest[:, up_end:])
        hidden = (silu(gate_sum * scale) * (rest[:, :hidden_cols] * scale)).astype(BF16)
        hid[stream * half + my_i] = hidden
        own = hid.at[stream * half + my_i]
        left = send_sem.at[event + 4 + stream]
        for target in range(2):
            for dc, dh, db in steps:
                last = dc == 0 and dh == 0 and db == 0
                if not (last and target == 0):
                    c, e, b = (
                        lax.rem(my_c + dc, groups),
                        lax.rem(my_h + dh + target, 2),
                        lax.rem(my_b + db, 2),
                    )
                    landed = late_sem.at[late + stream] if last else recv_sem.at[event + 4 + stream]
                    remote(own, own, "kv", device_at(c, target, e, b), left, landed).start()

    def ffn_sent(event, bufs, hid):
        for buf, at in ((bufs[1], event), (bufs[3], event + 2)):
            for cond, count in ((owner, n_kv - 2), (jnp.logical_not(owner), n_kv)):
                block = buf.at[pl.ds(0, count)]
                sent.append(
                    (cond, remote(block, block, "kv", kv, send_sem.at[at], recv_sem.at[at]))
                )
        for stream in range(2):
            block = hid.at[pl.ds(0, n_kv - 1)]
            at = event + 4 + stream
            sent.append((owner, remote(block, block, "kv", kv, send_sem.at[at], recv_sem.at[at])))

    def ffn_arrive(event, late, stream, hid):
        at = event + 4 + stream
        block = hid.at[pl.ds(0, half - 1)]
        remote(block, block, "kv", kv, send_sem.at[at], recv_sem.at[at]).wait_recv()
        own = hid.at[0]
        pl.when(jnp.logical_not(owner))(
            remote(own, own, "kv", kv, send_sem.at[at], late_sem.at[late + stream]).wait_recv
        )

    smalls[0].wait()
    own = res_all.at[tp]
    every = send_tp(0, lambda off: own, lambda off: own, res_all.at[pl.ds(0, n_tp - 1)])
    for load in loads[3:]:
        load.start()
    state_load = pltpu.make_async_copy(state_hbm, state, in_sem)
    state_load.start()
    for copy in smalls[1:]:
        copy.wait()
    decay_exp = jnp.exp(rate_ref[...])
    extra_weight = (
        dot_first(beta_ref[...], place_heads(beta_ref.shape[0], tp * heads, 0, heads))
        + dot_first(decay_ref[...], place_heads(beta_ref.shape[0], tp * heads, heads, heads))
    ).astype(BF16)
    with ns("tp_gather"):
        every.wait_recv()
        pieces = [res_all[source].astype(F32) for source in range(n_tp)]
        whole = jnp.concatenate(pieces, axis=1)

    first_bufs = (s1a, r1a, s1b, r1b)
    residual = [rows_of(whole, stream) for stream in range(2)]
    loads[0].wait()
    loads[1].wait()
    with ns("f1_in"):
        for stream in ORDER:
            ffn_in(1, stream, residual[stream], gain_first_ref, gate1, up1, first_bufs)
    for stream in ORDER:
        pl.when(owner)(functools.partial(ffn_mid, 1, 0, stream, first_bufs, hid1))
    ffn_sent(1, first_bufs, hid1)
    def first_out(stream):
        with ns("f1_ag%d" % stream):
            ffn_arrive(1, 0, stream, hid1)
        return share(7 + stream, stream, dot(flat(hid1, stream), down1[...]), par1)

    after_first = [None, None]

    def mixer_in(stream, shared):
        with ns("exch1_%d" % stream):
            branch = join(shared, stream, par1)
        kept = (residual[stream] + 0.5 * branch).astype(BF16).astype(F32)
        after_first[stream] = kept
        scaled = (kept * gain_mixer_ref[...]).astype(BF16)
        with ns("m_in"):
            put(sma, stream, 0, dot(scaled, wq[...]))
            put(sma, stream, key_cols, dot(scaled, wk[...]))
            put(sma, stream, 2 * key_cols, dot(scaled, extra_weight) + square_lanes(kept))
            scatter(9, stream, sma, rma)
            put(smb, stream, 0, dot(scaled, wv[...]))
            scatter(10, stream, smb, rmb)
            put(smc, stream, 0, dot(scaled, wo[...]))
            scatter(11, stream, smc, rmc)

    for load in loads[2:7]:
        load.wait()
    shared = first_out(ORDER[0])
    later = first_out(ORDER[1])
    mixer_in(ORDER[0], shared)
    mixer_in(ORDER[1], later)

    with ns("m_rs_a"):
        keys_sum = collect(9, sma, rma)
    extra = keys_sum[:, 2 * key_cols :]
    scale = row_scale(extra)
    for head in range(key_heads):
        for slot, start, factor in (
            (head, head * size, size ** (-0.5)),
            (key_heads + head, key_cols + head * size, 1.0),
        ):
            act = silu(keys_sum[:, start : start + size] * scale)
            unit = act * lax.rsqrt(jnp.sum(act * act, axis=1, keepdims=True) + EPS)
            qk_rows[:, slot, :] = unit * factor
    gates = extra * scale
    beta_pre = gates[:, :heads]
    decay_pre = gates[:, heads : 2 * heads] + bias_ref[...]
    beta_gate = 1.0 / (1.0 + jnp.exp(-beta_pre))
    softplus = jnp.maximum(decay_pre, 0.0) + jnp.log1p(jnp.exp(-jnp.abs(decay_pre)))
    decay_gate = jnp.exp(-decay_exp * softplus)
    for head in range(heads):
        dec_rows[:, head, :] = jnp.broadcast_to(decay_gate[:, head : head + 1], (own_rows, size))

    def look(row, carry):
        columns = qk_rows[row].T
        for head in range(heads):
            kh = head // repeat
            key_col = columns[:, key_heads + kh : key_heads + kh + 1]
            query_col = columns[:, kh : kh + 1]
            old = state[row, head]
            pred_rows[row, head : head + 1, :] = jnp.sum(old * key_col, axis=0, keepdims=True)
            read_rows[row, head : head + 1, :] = jnp.sum(old * query_col, axis=0, keepdims=True)
        return carry

    with ns("look"):
        state_load.wait()
        lax.fori_loop(0, own_rows, look, 0, unroll=UNROLL)

    with ns("m_rs_b"):
        values = silu(collect(10, smb, rmb) * scale)
    with ns("m_rs_c"):
        out_gate = silu(collect(11, smc, rmc) * scale)
    with ns("m_norm"):
        for head in range(heads):
            kh = head // repeat
            cols = slice(head * size, (head + 1) * size)
            decay = decay_gate[:, head : head + 1]
            correction = beta_gate[:, head : head + 1] * (
                values[:, cols] - decay * pred_rows[:, head, :]
            )
            val_rows[:, head, :] = correction
            match = jnp.sum(
                qk_rows[:, kh, :] * qk_rows[:, key_heads + kh, :], axis=1, keepdims=True
            )
            reading = decay * read_rows[:, head, :] + match * correction
            mean = jnp.mean(reading * reading, axis=1, keepdims=True)
            normed = reading * lax.rsqrt(mean + EPS) * head_gain_ref[...]
            nrm[my_j, :, cols] = (normed * out_gate[:, cols]).astype(BF16)
        spread(12, 2, nrm)

    def mixer_out(stream):
        with ns("m_ag%d" % stream):
            arrive(12, 2, stream, nrm)
        return share(14 + stream, stream, dot(flat(nrm, stream), wout[...]), parm)

    second_bufs = (s2a, r2a, s2b, r2b)
    after_mixer = [None, None]

    def second_in(stream, shared):
        with ns("exch2_%d" % stream):
            branch = join(shared, stream, parm)
        kept = (after_first[stream] + branch).astype(BF16).astype(F32)
        after_mixer[stream] = kept
        kept_rows[stream] = kept
        with ns("f2_in"):
            ffn_in(16, stream, kept, gain_second_ref, gate2, up2, second_bufs)

    for load in loads[7:10]:
        load.wait()
    shared = mixer_out(ORDER[0])
    second_in(ORDER[0], shared)
    second_in(ORDER[1], mixer_out(ORDER[1]))

    def update(row, carry):
        columns = qk_rows[row].T
        row_dec, row_vals = dec_rows[row], val_rows[row]
        for head in range(heads):
            kh = head // repeat
            key_col = columns[:, key_heads + kh : key_heads + kh + 1]
            state[row, head] = (
                state[row, head] * row_dec[head : head + 1, :]
                + key_col * row_vals[head : head + 1, :]
            )
        return carry

    for stream in ORDER:
        pl.when(owner)(functools.partial(ffn_mid, 16, 4, stream, second_bufs, hid2))
    ffn_sent(16, second_bufs, hid2)
    loads[10].wait()
    tile = min(LANES, depth)
    per = tile // piece

    def tile_of(ref, stream, place):
        if tile == depth:
            return ref.at[stream]
        return ref.at[stream, :, pl.ds(pl.multiple_of((place // per) * tile, tile), tile)]

    finals = []
    for stream in ORDER:
        with ns("f2_ag%d" % stream):
            ffn_arrive(16, 4, stream, hid2)
        product[stream] = dot(flat(hid2, stream), down2[...]).astype(BF16)
        every = send_tp(
            22 + stream,
            lambda off: tile_of(product, stream, lax.rem(tp + off, n_tp)),
            lambda off: fin_recv.at[stream, off],
            fin_recv.at[stream, pl.ds(1, n_tp - 1)],
        )
        finals.append((stream, every))

    with ns("update"):
        lax.fori_loop(0, own_rows, update, 0, unroll=UNROLL)

    for stream, every in finals:
        with ns("fin%d" % stream):
            every.wait_recv()
            branch = tile_of(product, stream, tp)[...].astype(F32)
            for off in range(1, n_tp):
                branch = branch + fin_recv[stream, off].astype(F32)
        wide = tile_of(kept_rows, stream, tp)[...] + 0.5 * branch
        done = wide[:, :piece]
        for part in range(1, per):
            mine = wide[:, part * piece : (part + 1) * piece]
            done = jnp.where(lax.rem(tp, per) == part, mine, done)
        for j in range(half):
            start = start_of(stream, j)
            res_out_ref[start : start + own_rows] = done[j * own_rows : (j + 1) * own_rows].astype(
                BF16
            )

    for cond, every in sent:
        if cond is None:
            every.wait_send()
        else:
            pl.when(cond)(every.wait_send)


def finish(res_ref, state_ref, res_out, state_out, sem):
    rows = state_ref.shape[0]
    copies = [
        pltpu.make_async_copy(state_ref.at[row], state_out.at[row], sem.at[row])
        for row in range(rows)
    ]
    copies.append(pltpu.make_async_copy(res_ref, res_out, sem.at[rows]))
    for copy in copies:
        copy.start()
    for copy in copies:
        copy.wait()


def place_heads(rows, first, lane_start, count):
    row = lax.broadcasted_iota(jnp.int32, (rows, LANES), 0)
    col = lax.broadcasted_iota(jnp.int32, (rows, LANES), 1)
    inside = (col >= lane_start) & (col < lane_start + count)
    hit = inside & (row == col - lane_start + first)
    return jnp.where(hit, 1.0, 0.0).astype(F32).astype(BF16)


def body(
    n_kv,
    n_tp,
    residual_in,
    delta_state,
    norm_gain_first,
    gate_first,
    up_first,
    down_first,
    norm_gain_mixer,
    query_weight,
    key_weight,
    value_weight,
    output_gate_weight,
    beta_weight,
    decay_weight,
    decay_rate,
    decay_bias,
    head_gain,
    out_weight,
    norm_gain_second,
    gate_second,
    up_second,
    down_second,
):
    batch, piece = residual_in.shape
    depth, hidden = gate_first.shape
    own_rows, heads, size, _ = delta_state.shape
    key_cols = query_weight.shape[1]
    val_cols = value_weight.shape[1]
    key_heads = key_cols // size
    hp = pad_lanes(hidden)

    def like(x):
        return pltpu.VMEM(x.shape, x.dtype)

    def slots(cols, times=1):
        return pltpu.VMEM((times * n_kv, own_rows, cols), BF16)


    def row_buf(count):
        return pltpu.VMEM((own_rows, count, size), F32)

    tp_slots = pltpu.VMEM((2, n_tp, batch // 2, depth), BF16)
    ffn_bufs = [
        slots(hp),
        slots(hp, 2),
        slots(hp + LANES),
        slots(hp + LANES, 2),
        slots(hidden),
        tp_slots,
    ]
    wide = 2 * key_cols + LANES
    mixer_bufs = [
        slots(wide),
        slots(wide),
        slots(val_cols),
        slots(val_cols),
        slots(val_cols),
        slots(val_cols),
        slots(heads * size),
        tp_slots,
    ]
    big = (
        gate_first,
        up_first,
        down_first,
        query_weight,
        key_weight,
        value_weight,
        output_gate_weight,
        out_weight,
        gate_second,
        up_second,
        down_second,
    )
    small = (
        residual_in,
        norm_gain_first[None, :],
        norm_gain_mixer[None, :],
        norm_gain_second[None, :],
        beta_weight.T,
        decay_weight.T,
        decay_rate[None, :],
        decay_bias[None, :],
        head_gain[None, :],
    )
    vmem = pl.BlockSpec(memory_space=pltpu.VMEM)
    hbm = pl.BlockSpec(memory_space=pl.ANY)
    done = pl.pallas_call(
        functools.partial(kernel, n_kv, n_tp),
        out_shape=(
            pltpu.VMEM(residual_in.shape, BF16),
            pltpu.VMEM(delta_state.shape, F32),
        ),
        in_specs=[hbm] * (len(small) + 1 + len(big)),
        out_specs=(vmem, vmem),
        scratch_shapes=[like(x) for x in (*small[1:], *big)]
        + [pltpu.VMEM((n_tp, batch, piece), BF16)]
        + ffn_bufs
        + mixer_bufs
        + ffn_bufs[:-1]
        + [
            pltpu.VMEM((2, batch // 2, depth), F32),
            pltpu.VMEM((2, batch // 2, depth), BF16),
            pltpu.VMEM((2, n_tp, batch // 2, min(LANES, depth)), BF16),
        ]
        + [row_buf(2 * key_heads), row_buf(heads), row_buf(heads), row_buf(heads), row_buf(heads)]
        + [
            pltpu.SemaphoreType.DMA((len(big),)),
            pltpu.SemaphoreType.DMA((len(small),)),
            pltpu.SemaphoreType.DMA,
            pltpu.SemaphoreType.DMA((24,)),
            pltpu.SemaphoreType.DMA((24,)),
            pltpu.SemaphoreType.DMA((6,)),
        ],
        compiler_params=pltpu.CompilerParams(
            collective_id=0, has_side_effects=True, vmem_limit_bytes=58 * 1024 * 1024
        ),
        name="layer",
    )(*small, delta_state, *big)
    return pl.pallas_call(
        finish,
        out_shape=(
            jax.ShapeDtypeStruct(residual_in.shape, BF16),
            jax.ShapeDtypeStruct(delta_state.shape, F32),
        ),
        in_specs=[vmem, vmem],
        out_specs=(hbm, hbm),
        scratch_shapes=[pltpu.SemaphoreType.DMA((own_rows + 1,))],
        compiler_params=pltpu.CompilerParams(vmem_limit_bytes=1024 * 1024),
        name="finish",
    )(*done)


def solution(mesh):
    placed = (
        P(None, ("kv", "tp")),
        P("kv", "tp", None, None),
        P("kv"),
        P("kv", "tp"),
        P("kv", "tp"),
        P("tp", "kv"),
        P("kv"),
        P("kv", "tp"),
        P("kv", "tp"),
        P("kv", "tp"),
        P("kv", "tp"),
        P("kv", None),
        P("kv", None),
        P("tp"),
        P("tp"),
        P(),
        P("tp", "kv"),
        P("kv"),
        P("kv", "tp"),
        P("kv", "tp"),
        P("tp", "kv"),
    )
    return jax.shard_map(
        functools.partial(body, mesh.shape["kv"], mesh.shape["tp"]),
        mesh=mesh,
        in_specs=placed,
        out_specs=(P(None, ("kv", "tp")), P("kv", "tp", None, None)),
        check_vma=False,
    )
```

```python
import functools

import jax
import jax.numpy as jnp
from jax import lax
from jax.experimental import pallas as pl
from jax.experimental.pallas import tpu as pltpu
from jax.sharding import PartitionSpec as P

EPS = 1e-06
GROUP = 8
UNROLL = 8
ORDER = (0, 1)
LANES = 128
BF16 = jnp.bfloat16
F32 = jnp.float32
ns = jax.named_scope


def pad_lanes(size):
    return -(-size // LANES) * LANES


def silu(v):
    return v / (1.0 + jnp.exp(-v))


def dot(a, b):
    return jnp.dot(a, b, preferred_element_type=F32)


def dot_first(a, b):
    return lax.dot_general(a, b, (((0,), (0,)), ((), ())), preferred_element_type=F32)


def kernel(
    n_kv,
    n_tp,
    res_hbm,
    gain_first_hbm,
    gain_mixer_hbm,
    gain_second_hbm,
    beta_hbm,
    decay_hbm,
    rate_hbm,
    bias_hbm,
    head_gain_hbm,
    state_hbm,
    gate1_hbm,
    up1_hbm,
    down1_hbm,
    wq_hbm,
    wk_hbm,
    wv_hbm,
    wo_hbm,
    out_hbm,
    gate2_hbm,
    up2_hbm,
    down2_hbm,
    res_out_ref,
    state,
    gain_first_ref,
    gain_mixer_ref,
    gain_second_ref,
    beta_ref,
    decay_ref,
    rate_ref,
    bias_ref,
    head_gain_ref,
    gate1,
    up1,
    down1,
    wq,
    wk,
    wv,
    wo,
    wout,
    gate2,
    up2,
    down2,
    res_all,
    s1a,
    r1a,
    s1b,
    r1b,
    hid1,
    par1,
    sma,
    rma,
    smb,
    rmb,
    smc,
    rmc,
    nrm,
    parm,
    s2a,
    r2a,
    s2b,
    r2b,
    hid2,
    kept_rows,
    product,
    fin_recv,
    qk_rows,
    val_rows,
    dec_rows,
    pred_rows,
    read_rows,
    w_sem,
    small_sem,
    in_sem,
    send_sem,
    recv_sem,
    late_sem,
):
    kv = lax.axis_index("kv")
    tp = lax.axis_index("tp")
    _, batch, piece = res_all.shape
    depth = gate1.shape[0]
    width = depth * n_kv
    own_rows = batch // n_kv
    heads = state.shape[1]
    size = state.shape[2]
    key_cols = wq.shape[1]
    key_heads = key_cols // size
    repeat = heads // key_heads
    half = n_kv // 2
    groups = n_kv // GROUP

    turned = lax.rem(kv + GROUP - 2, GROUP)
    my_c = kv // GROUP
    my_s = turned // 4
    my_e = lax.rem(turned, 4) // 2
    my_b = lax.rem(turned, 2)
    my_i = my_c * 4 + my_e * 2 + my_b
    my_j = my_s * half + my_i
    owner = my_s == 0

    def device_at(c, stream, e, b):
        return c * GROUP + lax.rem(stream * 4 + e * 2 + b + 2, GROUP)

    def start_of(stream, j):
        return ((j // 4) * GROUP + (stream * 4 + j % 4 + 2) % GROUP) * own_rows

    def rows_of(value, stream):
        parts = [value[start_of(stream, j) : start_of(stream, j) + own_rows] for j in range(half)]
        return jnp.concatenate(parts, axis=0)

    weight_pairs = (
        (gate1_hbm, gate1),
        (up1_hbm, up1),
        (down1_hbm, down1),
        (wq_hbm, wq),
        (wk_hbm, wk),
        (wv_hbm, wv),
        (wo_hbm, wo),
        (out_hbm, wout),
        (gate2_hbm, gate2),
        (up2_hbm, up2),
        (down2_hbm, down2),
    )
    loads = [
        pltpu.make_async_copy(src, dst, w_sem.at[i]) for i, (src, dst) in enumerate(weight_pairs)
    ]
    small_pairs = (
        (res_hbm, res_all.at[tp]),
        (gain_first_hbm, gain_first_ref),
        (gain_mixer_hbm, gain_mixer_ref),
        (gain_second_hbm, gain_second_ref),
        (beta_hbm, beta_ref),
        (decay_hbm, decay_ref),
        (rate_hbm, rate_ref),
        (bias_hbm, bias_ref),
        (head_gain_hbm, head_gain_ref),
    )
    smalls = [
        pltpu.make_async_copy(src, dst, small_sem.at[i])
        for i, (src, dst) in enumerate(small_pairs)
    ]
    smalls[0].start()
    barrier = pltpu.get_barrier_semaphore()
    for off in range(1, n_tp):
        pl.semaphore_signal(
            barrier,
            inc=1,
            device_id={"tp": lax.rem(tp + off, n_tp)},
            device_id_type=pl.DeviceIdType.MESH,
        )

    @pl.when(owner)
    def greet():
        for off in range(1, n_kv):
            pl.semaphore_signal(
                barrier,
                inc=1,
                device_id={"kv": lax.rem(kv + off, n_kv)},
                device_id_type=pl.DeviceIdType.MESH,
            )

    for copy in smalls[1:] + loads[:3]:
        copy.start()
    with ns("barrier"):
        pl.semaphore_wait(barrier, n_tp - 1 + half - 1 + my_s)

    def remote(src, dst, axis, peer, left, landed):
        return pltpu.make_async_remote_copy(
            src_ref=src,
            dst_ref=dst,
            send_sem=left,
            recv_sem=landed,
            device_id={axis: peer},
            device_id_type=pl.DeviceIdType.MESH,
        )

    sent = []

    def settle():
        for cond, every in sent:
            if cond is None:
                every.wait_send()
            else:
                pl.when(cond)(every.wait_send)
        sent.clear()

    def send_tp(event, src_of, dst_of, block):
        sems = send_sem.at[event], recv_sem.at[event]
        for off in range(1, n_tp):
            peer = lax.rem(tp + off, n_tp)
            remote(src_of(off), dst_of(off), "tp", peer, *sems).start()
        every = remote(block, block, "tp", tp, *sems)
        sent.append((None, every))
        return every

    steps = [
        (dc, dh, db) for dc in range(groups - 1, -1, -1) for dh in (1, 0) for db in (1, 0)
    ]
    my_h = lax.rem(my_e + my_s, 2)

    def each_kv(stream, make):
        turn = lax.rem(stream + 2 - my_s, 2)
        for dc, dh, db in steps:
            c, b = lax.rem(my_c + dc, groups), lax.rem(my_b + db, 2)
            e = lax.rem(my_h + dh + stream, 2)
            last = dc == 0 and dh == 0 and db == 0
            copy = make(
                dc * GROUP + turn * 4 + dh * 2 + db,
                device_at(c, stream, e, b),
                c * 4 + e * 2 + b,
                last,
            )
            if last:
                pl.when(my_s != stream)(copy.start)
            else:
                copy.start()

    def scatter(event, stream, sends, receives):
        sems = send_sem.at[event], recv_sem.at[event]
        each_kv(
            stream,
            lambda index, peer, j, last: remote(
                sends.at[stream * half + j], receives.at[index], "kv", peer, *sems
            ),
        )

    def collect(event, sends, receives):
        block = receives.at[pl.ds(1, n_kv - 1)]
        every = remote(block, block, "kv", kv, send_sem.at[event], recv_sem.at[event])
        every.wait_recv()
        sent.append((None, every))
        total = sends[my_j].astype(F32)
        for index in range(1, n_kv):
            total = total + receives[index].astype(F32)
        return total

    def spread(event, late, slots):
        own = slots.at[my_j]
        left = send_sem.at[event]
        for stream in range(2):
            each_kv(
                stream,
                lambda index, peer, j, last: remote(
                    own,
                    own,
                    "kv",
                    peer,
                    left,
                    late_sem.at[late + my_s] if last else recv_sem.at[event + my_s],
                ),
            )
        block = slots.at[pl.ds(0, n_kv - 1)]
        sent.append((None, remote(block, block, "kv", kv, left, recv_sem.at[event])))

    def arrive(event, late, stream, slots):
        left = send_sem.at[event]
        block = slots.at[pl.ds(0, half - 1)]
        remote(block, block, "kv", kv, left, recv_sem.at[event + stream]).wait_recv()
        own = slots.at[0]
        pl.when(my_s != stream)(
            remote(own, own, "kv", kv, left, late_sem.at[late + stream]).wait_recv
        )

    def put(ref, stream, offset, value):
        cols = value.shape[1]
        ref[stream * half : (stream + 1) * half, :, offset : offset + cols] = value.reshape(
            half, own_rows, cols
        ).astype(BF16)

    def square_lanes(residual):
        squares = jnp.sum(residual * residual, axis=1, keepdims=True)
        high = squares.astype(BF16).astype(F32)
        lane = lax.broadcasted_iota(jnp.int32, (residual.shape[0], LANES), 1)
        return jnp.where(lane == 64, high, jnp.where(lane == 65, squares - high, 0.0))

    def row_scale(extra):
        squares = extra[:, 64:65] + extra[:, 65:66]
        return lax.rsqrt(squares / width + EPS)

    def flat(slots, stream):
        both = slots[stream * half : (stream + 1) * half].astype(F32)
        return both.reshape(half * own_rows, both.shape[2]).astype(BF16)

    def share(event, stream, value, slots):
        slots[stream, tp] = value.astype(BF16)
        own = slots.at[stream, tp]
        block = slots.at[stream, pl.ds(0, n_tp - 1)]
        return send_tp(event, lambda off: own, lambda off: own, block)

    def join(every, stream, slots):
        every.wait_recv()
        total = slots[stream, 0].astype(F32)
        for other in range(1, n_tp):
            total = total + slots[stream, other].astype(F32)
        return total

    def to_owners(event, stream, sends, receives):
        sems = send_sem.at[event], recv_sem.at[event + stream]
        each_kv(
            0,
            lambda index, peer, j, last: remote(
                sends.at[stream * half + j], receives.at[stream * n_kv + index], "kv", peer, *sems
            ),
        )

    def owned(event, stream, sends, receives):
        block = receives.at[pl.ds(stream * n_kv + 1, n_kv - 1)]
        remote(block, block, "kv", kv, send_sem.at[event], recv_sem.at[event + stream]).wait_recv()
        total = sends[stream * half + my_i].astype(F32)
        for index in range(1, n_kv):
            total = total + receives[stream * n_kv + index].astype(F32)
        return total

    def ffn_in(event, stream, residual, gain_ref, w_gate, w_up, bufs):
        send_a, recv_a, send_b, recv_b = bufs
        up_end = pad_lanes(w_gate.shape[1])
        scaled = (residual * gain_ref[...]).astype(BF16)
        put(send_a, stream, 0, dot(scaled, w_gate[...]))
        to_owners(event, stream, send_a, recv_a)
        put(send_b, stream, 0, dot(scaled, w_up[...]))
        put(send_b, stream, up_end, square_lanes(residual))
        to_owners(event + 2, stream, send_b, recv_b)

    def ffn_mid(event, late, stream, bufs, hid):
        send_a, recv_a, send_b, recv_b = bufs
        hidden_cols = hid.shape[-1]
        up_end = pad_lanes(hidden_cols)
        with ns("f_rs_a"):
            gate_sum = owned(event, stream, send_a, recv_a)[:, :hidden_cols]
        with ns("f_rs_b"):
            rest = owned(event + 2, stream, send_b, recv_b)
        scale = row_scale(rest[:, up_end:])
        hidden = (silu(gate_sum * scale) * (rest[:, :hidden_cols] * scale)).astype(BF16)
        hid[stream * half + my_i] = hidden
        own = hid.at[stream * half + my_i]
        left = send_sem.at[event + 4 + stream]
        for target in range(2):
            for dc, dh, db in steps:
                last = dc == 0 and dh == 0 and db == 0
                if not (last and target == 0):
                    c, e, b = (
                        lax.rem(my_c + dc, groups),
                        lax.rem(my_h + dh + target, 2),
                        lax.rem(my_b + db, 2),
                    )
                    landed = late_sem.at[late + stream] if last else recv_sem.at[event + 4 + stream]
                    remote(own, own, "kv", device_at(c, target, e, b), left, landed).start()

    def ffn_sent(event, bufs, hid):
        for buf, at in ((bufs[1], event), (bufs[3], event + 2)):
            for cond, count in ((owner, n_kv - 2), (jnp.logical_not(owner), n_kv)):
                block = buf.at[pl.ds(0, count)]
                sent.append(
                    (cond, remote(block, block, "kv", kv, send_sem.at[at], recv_sem.at[at]))
                )
        for stream in range(2):
            block = hid.at[pl.ds(0, n_kv - 1)]
            at = event + 4 + stream
            sent.append((owner, remote(block, block, "kv", kv, send_sem.at[at], recv_sem.at[at])))

    def ffn_arrive(event, late, stream, hid):
        at = event + 4 + stream
        block = hid.at[pl.ds(0, half - 1)]
        remote(block, block, "kv", kv, send_sem.at[at], recv_sem.at[at]).wait_recv()
        own = hid.at[0]
        pl.when(jnp.logical_not(owner))(
            remote(own, own, "kv", kv, send_sem.at[at], late_sem.at[late + stream]).wait_recv
        )

    smalls[0].wait()
    own = res_all.at[tp]
    every = send_tp(0, lambda off: own, lambda off: own, res_all.at[pl.ds(0, n_tp - 1)])
    for load in loads[3:]:
        load.start()
    state_load = pltpu.make_async_copy(state_hbm, state, in_sem)
    state_load.start()
    for copy in smalls[1:]:
        copy.wait()
    decay_exp = jnp.exp(rate_ref[...])
    extra_weight = (
        dot_first(beta_ref[...], place_heads(beta_ref.shape[0], tp * heads, 0, heads))
        + dot_first(decay_ref[...], place_heads(beta_ref.shape[0], tp * heads, heads, heads))
    ).astype(BF16)
    with ns("tp_gather"):
        every.wait_recv()
        pieces = [res_all[source].astype(F32) for source in range(n_tp)]
        whole = jnp.concatenate(pieces, axis=1)

    first_bufs = (s1a, r1a, s1b, r1b)
    residual = [rows_of(whole, stream) for stream in range(2)]
    loads[0].wait()
    loads[1].wait()
    with ns("f1_in"):
        for stream in ORDER:
            ffn_in(1, stream, residual[stream], gain_first_ref, gate1, up1, first_bufs)
    for stream in ORDER:
        pl.when(owner)(functools.partial(ffn_mid, 1, 0, stream, first_bufs, hid1))
    ffn_sent(1, first_bufs, hid1)
    def first_out(stream):
        with ns("f1_ag%d" % stream):
            ffn_arrive(1, 0, stream, hid1)
        return share(7 + stream, stream, dot(flat(hid1, stream), down1[...]), par1)

    after_first = [None, None]

    def mixer_in(stream, shared):
        with ns("exch1_%d" % stream):
            branch = join(shared, stream, par1)
        kept = (residual[stream] + 0.5 * branch).astype(BF16).astype(F32)
        after_first[stream] = kept
        scaled = (kept * gain_mixer_ref[...]).astype(BF16)
        with ns("m_in"):
            put(sma, stream, 0, dot(scaled, wq[...]))
            put(sma, stream, key_cols, dot(scaled, wk[...]))
            put(sma, stream, 2 * key_cols, dot(scaled, extra_weight) + square_lanes(kept))
            scatter(9, stream, sma, rma)
            put(smb, stream, 0, dot(scaled, wv[...]))
            scatter(10, stream, smb, rmb)
            put(smc, stream, 0, dot(scaled, wo[...]))
            scatter(11, stream, smc, rmc)

    for load in loads[2:7]:
        load.wait()
    shared = first_out(ORDER[0])
    later = first_out(ORDER[1])
    mixer_in(ORDER[0], shared)
    mixer_in(ORDER[1], later)

    with ns("m_rs_a"):
        keys_sum = collect(9, sma, rma)
    extra = keys_sum[:, 2 * key_cols :]
    scale = row_scale(extra)
    for head in range(key_heads):
        for slot, start, factor in (
            (head, head * size, size ** (-0.5)),
            (key_heads + head, key_cols + head * size, 1.0),
        ):
            act = silu(keys_sum[:, start : start + size] * scale)
            unit = act * lax.rsqrt(jnp.sum(act * act, axis=1, keepdims=True) + EPS)
            qk_rows[:, slot, :] = unit * factor
    gates = extra * scale
    beta_pre = gates[:, :heads]
    decay_pre = gates[:, heads : 2 * heads] + bias_ref[...]
    beta_gate = 1.0 / (1.0 + jnp.exp(-beta_pre))
    softplus = jnp.maximum(decay_pre, 0.0) + jnp.log1p(jnp.exp(-jnp.abs(decay_pre)))
    decay_gate = jnp.exp(-decay_exp * softplus)
    for head in range(heads):
        dec_rows[:, head, :] = jnp.broadcast_to(decay_gate[:, head : head + 1], (own_rows, size))

    def look(row, carry):
        columns = qk_rows[row].T
        for head in range(heads):
            kh = head // repeat
            key_col = columns[:, key_heads + kh : key_heads + kh + 1]
            query_col = columns[:, kh : kh + 1]
            old = state[row, head]
            pred_rows[row, head : head + 1, :] = jnp.sum(old * key_col, axis=0, keepdims=True)
            read_rows[row, head : head + 1, :] = jnp.sum(old * query_col, axis=0, keepdims=True)
        return carry

    with ns("look"):
        state_load.wait()
        lax.fori_loop(0, own_rows, look, 0, unroll=UNROLL)

    with ns("m_rs_b"):
        values = silu(collect(10, smb, rmb) * scale)
    with ns("m_rs_c"):
        out_gate = silu(collect(11, smc, rmc) * scale)
    with ns("m_norm"):
        for head in range(heads):
            kh = head // repeat
            cols = slice(head * size, (head + 1) * size)
            decay = decay_gate[:, head : head + 1]
            correction = beta_gate[:, head : head + 1] * (
                values[:, cols] - decay * pred_rows[:, head, :]
            )
            val_rows[:, head, :] = correction
            match = jnp.sum(
                qk_rows[:, kh, :] * qk_rows[:, key_heads + kh, :], axis=1, keepdims=True
            )
            reading = decay * read_rows[:, head, :] + match * correction
            mean = jnp.mean(reading * reading, axis=1, keepdims=True)
            normed = reading * lax.rsqrt(mean + EPS) * head_gain_ref[...]
            nrm[my_j, :, cols] = (normed * out_gate[:, cols]).astype(BF16)
        spread(12, 2, nrm)
        late_send = sent.pop()
    settle()
    sent.append(late_send)

    def mixer_out(stream):
        with ns("m_ag%d" % stream):
            arrive(12, 2, stream, nrm)
        return share(14 + stream, stream, dot(flat(nrm, stream), wout[...]), parm)

    second_bufs = (s2a, r2a, s2b, r2b)
    after_mixer = [None, None]

    def second_in(stream, shared):
        with ns("exch2_%d" % stream):
            branch = join(shared, stream, parm)
        kept = (after_first[stream] + branch).astype(BF16).astype(F32)
        after_mixer[stream] = kept
        kept_rows[stream] = kept
        with ns("f2_in"):
            ffn_in(1, stream, kept, gain_second_ref, gate2, up2, second_bufs)

    for load in loads[7:10]:
        load.wait()
    shared = mixer_out(ORDER[0])
    second_in(ORDER[0], shared)
    second_in(ORDER[1], mixer_out(ORDER[1]))

    def update(row, carry):
        columns = qk_rows[row].T
        row_dec, row_vals = dec_rows[row], val_rows[row]
        for head in range(heads):
            kh = head // repeat
            key_col = columns[:, key_heads + kh : key_heads + kh + 1]
            state[row, head] = (
                state[row, head] * row_dec[head : head + 1, :]
                + key_col * row_vals[head : head + 1, :]
            )
        return carry

    for stream in ORDER:
        pl.when(owner)(functools.partial(ffn_mid, 1, 0, stream, second_bufs, hid2))
    ffn_sent(1, second_bufs, hid2)
    loads[10].wait()
    tile = min(LANES, depth)
    per = tile // piece

    def tile_of(ref, stream, place):
        if tile == depth:
            return ref.at[stream]
        return ref.at[stream, :, pl.ds(pl.multiple_of((place // per) * tile, tile), tile)]

    finals = []
    for stream in ORDER:
        with ns("f2_ag%d" % stream):
            ffn_arrive(1, 0, stream, hid2)
        product[stream] = dot(flat(hid2, stream), down2[...]).astype(BF16)
        every = send_tp(
            16 + stream,
            lambda off: tile_of(product, stream, lax.rem(tp + off, n_tp)),
            lambda off: fin_recv.at[stream, off],
            fin_recv.at[stream, pl.ds(1, n_tp - 1)],
        )
        finals.append((stream, every))

    final_sends = sent[-2:]
    del sent[-2:]
    settle()
    sent.extend(final_sends)
    with ns("update"):
        lax.fori_loop(0, own_rows, update, 0, unroll=UNROLL)

    for stream, every in finals:
        with ns("fin%d" % stream):
            every.wait_recv()
            branch = tile_of(product, stream, tp)[...].astype(F32)
            for off in range(1, n_tp):
                branch = branch + fin_recv[stream, off].astype(F32)
        wide = tile_of(kept_rows, stream, tp)[...] + 0.5 * branch
        done = wide[:, :piece]
        for part in range(1, per):
            mine = wide[:, part * piece : (part + 1) * piece]
            done = jnp.where(lax.rem(tp, per) == part, mine, done)
        for j in range(half):
            start = start_of(stream, j)
            res_out_ref[start : start + own_rows] = done[j * own_rows : (j + 1) * own_rows].astype(
                BF16
            )

    settle()


def finish(res_ref, state_ref, res_out, state_out, sem):
    rows = state_ref.shape[0]
    copies = [
        pltpu.make_async_copy(state_ref.at[row], state_out.at[row], sem.at[row])
        for row in range(rows)
    ]
    copies.append(pltpu.make_async_copy(res_ref, res_out, sem.at[rows]))
    for copy in copies:
        copy.start()
    for copy in copies:
        copy.wait()


def place_heads(rows, first, lane_start, count):
    row = lax.broadcasted_iota(jnp.int32, (rows, LANES), 0)
    col = lax.broadcasted_iota(jnp.int32, (rows, LANES), 1)
    inside = (col >= lane_start) & (col < lane_start + count)
    hit = inside & (row == col - lane_start + first)
    return jnp.where(hit, 1.0, 0.0).astype(F32).astype(BF16)


def body(
    n_kv,
    n_tp,
    residual_in,
    delta_state,
    norm_gain_first,
    gate_first,
    up_first,
    down_first,
    norm_gain_mixer,
    query_weight,
    key_weight,
    value_weight,
    output_gate_weight,
    beta_weight,
    decay_weight,
    decay_rate,
    decay_bias,
    head_gain,
    out_weight,
    norm_gain_second,
    gate_second,
    up_second,
    down_second,
):
    batch, piece = residual_in.shape
    depth, hidden = gate_first.shape
    own_rows, heads, size, _ = delta_state.shape
    key_cols = query_weight.shape[1]
    val_cols = value_weight.shape[1]
    key_heads = key_cols // size
    hp = pad_lanes(hidden)

    def like(x):
        return pltpu.VMEM(x.shape, x.dtype)

    def slots(cols, times=1):
        return pltpu.VMEM((times * n_kv, own_rows, cols), BF16)


    def row_buf(count):
        return pltpu.VMEM((own_rows, count, size), F32)

    tp_slots = pltpu.VMEM((2, n_tp, batch // 2, depth), BF16)
    ffn_bufs = [
        slots(hp),
        slots(hp, 2),
        slots(hp + LANES),
        slots(hp + LANES, 2),
        slots(hidden),
        tp_slots,
    ]
    wide = 2 * key_cols + LANES
    mixer_bufs = [
        slots(wide),
        slots(wide),
        slots(val_cols),
        slots(val_cols),
        slots(val_cols),
        slots(val_cols),
        slots(heads * size),
        tp_slots,
    ]
    big = (
        gate_first,
        up_first,
        down_first,
        query_weight,
        key_weight,
        value_weight,
        output_gate_weight,
        out_weight,
        gate_second,
        up_second,
        down_second,
    )
    small = (
        residual_in,
        norm_gain_first[None, :],
        norm_gain_mixer[None, :],
        norm_gain_second[None, :],
        beta_weight.T,
        decay_weight.T,
        decay_rate[None, :],
        decay_bias[None, :],
        head_gain[None, :],
    )
    vmem = pl.BlockSpec(memory_space=pltpu.VMEM)
    hbm = pl.BlockSpec(memory_space=pl.ANY)
    done = pl.pallas_call(
        functools.partial(kernel, n_kv, n_tp),
        out_shape=(
            pltpu.VMEM(residual_in.shape, BF16),
            pltpu.VMEM(delta_state.shape, F32),
        ),
        in_specs=[hbm] * (len(small) + 1 + len(big)),
        out_specs=(vmem, vmem),
        scratch_shapes=[like(x) for x in (*small[1:], *big)]
        + [pltpu.VMEM((n_tp, batch, piece), BF16)]
        + ffn_bufs
        + mixer_bufs
        + ffn_bufs[:-1]
        + [
            pltpu.VMEM((2, batch // 2, depth), F32),
            pltpu.VMEM((2, batch // 2, depth), BF16),
            pltpu.VMEM((2, n_tp, batch // 2, min(LANES, depth)), BF16),
        ]
        + [row_buf(2 * key_heads), row_buf(heads), row_buf(heads), row_buf(heads), row_buf(heads)]
        + [
            pltpu.SemaphoreType.DMA((len(big),)),
            pltpu.SemaphoreType.DMA((len(small),)),
            pltpu.SemaphoreType.DMA,
            pltpu.SemaphoreType.DMA((18,)),
            pltpu.SemaphoreType.DMA((18,)),
            pltpu.SemaphoreType.DMA((4,)),
        ],
        compiler_params=pltpu.CompilerParams(
            collective_id=0, has_side_effects=True, vmem_limit_bytes=58 * 1024 * 1024
        ),
        name="layer",
    )(*small, delta_state, *big)
    return pl.pallas_call(
        finish,
        out_shape=(
            jax.ShapeDtypeStruct(residual_in.shape, BF16),
            jax.ShapeDtypeStruct(delta_state.shape, F32),
        ),
        in_specs=[vmem, vmem],
        out_specs=(hbm, hbm),
        scratch_shapes=[pltpu.SemaphoreType.DMA((own_rows + 1,))],
        compiler_params=pltpu.CompilerParams(vmem_limit_bytes=1024 * 1024),
        name="finish",
    )(*done)


def solution(mesh):
    placed = (
        P(None, ("kv", "tp")),
        P("kv", "tp", None, None),
        P("kv"),
        P("kv", "tp"),
        P("kv", "tp"),
        P("tp", "kv"),
        P("kv"),
        P("kv", "tp"),
        P("kv", "tp"),
        P("kv", "tp"),
        P("kv", "tp"),
        P("kv", None),
        P("kv", None),
        P("tp"),
        P("tp"),
        P(),
        P("tp", "kv"),
        P("kv"),
        P("kv", "tp"),
        P("kv", "tp"),
        P("tp", "kv"),
    )
    return jax.shard_map(
        functools.partial(body, mesh.shape["kv"], mesh.shape["tp"]),
        mesh=mesh,
        in_specs=placed,
        out_specs=(P(None, ("kv", "tp")), P("kv", "tp", None, None)),
        check_vma=False,
    )
```
